32 devices in a mesh: fs: 4 (over y, x), tp: 8 (over z, core).
Axes of the slice: x: 2, y: 2, z: 4, core: 2. Of those that a mesh axis runs over, the one named last changes fastest.
Arguments:
- tokens: bfloat16 [2048, 2048], P('fs', 'tp'), may hold values from -6 to 6
- norm_gain: float32 [2048], P('fs'), may hold values from 0.1 to 1.9
- gate_train: float32 [2048, 8192], P('fs', 'tp'), may hold values from -0.125 to 0.125
- up_train: float32 [2048, 8192], P('fs', 'tp'), may hold values from -0.125 to 0.125
- down_train: float32 [8192, 2048], P('fs', 'tp'), may hold values from -0.0625 to 0.0625
Outputs:
- gate_serve: bfloat16 [2048, 8192], P(None, 'tp')
- up_serve: bfloat16 [2048, 8192], P(None, 'tp')
- down_serve: bfloat16 [8192, 2048], P('tp')
- layer_out: bfloat16 [2048, 2048], P(('fs', 'tp'))
The draws below stay inside these ranges and needn't reach their ends.
All inputs are finite; a program needn't handle non-finite values.
Results may differ from the reference program's by a relative error of at most 0.024.
Values may be sent and summed in bfloat16 or wider, within the bound.
A program may use at most 64 MiB of HBM per device.

```python
import jax
import jax.numpy as jnp
from jax import lax

D = 2048
FF = 8192
TOKENS = 2048


def level_of(own_key, shape, pieces, low, top_value):
    level, own = 1.0, jax.random.fold_in(own_key, 6)
    for position, parts in pieces:
        steps = jnp.exp(jax.random.uniform(jax.random.fold_in(own, position), (parts,), jnp.float32, low / len(pieces), top_value / len(pieces)))
        level = level * jnp.repeat(steps, shape[position] // parts).reshape([-1 if axis == position else 1 for axis in range(len(shape))])
    return level


def centred(own_key, extent, deviation, limit, shards=(), held_as=jnp.bfloat16):
    loudness = level_of(own_key, extent, shards, -0.22, 0.18) if shards else 1.0
    result = jax.random.normal(own_key, extent, jnp.float32) * deviation * loudness
    return jnp.minimum(jnp.maximum(result, -limit), limit).astype(held_as)


def setup_inputs(seed: int = 0) -> dict:
    splits = jax.random.split(jax.random.key(seed), 6)
    tokens = centred(splits[0], (TOKENS, D), 1.0, 6.0, ((0, 4), (1, 8)))
    norm_gain = jnp.clip(1.0 + 0.18 * jax.random.normal(splits[1], (D,), jnp.float32), 0.1, 1.9)
    gate_train = centred(splits[2], (D, FF), D ** -0.5, 0.125, ((0, 4), (1, 8)), jnp.float32)
    up_train = centred(splits[3], (D, FF), D ** -0.5, 0.125, ((0, 4), (1, 8)), jnp.float32)
    down_train = centred(splits[4], (FF, D), FF ** -0.5, 0.0625, ((0, 4), (1, 8)), jnp.float32)
    return dict(tokens=tokens, norm_gain=norm_gain, gate_train=gate_train, up_train=up_train, down_train=down_train)


def reference(tokens, norm_gain, gate_train, up_train, down_train):
    gate_serve = (norm_gain[:, None] * gate_train).astype(jnp.bfloat16)
    up_serve = (norm_gain[:, None] * up_train).astype(jnp.bfloat16)
    down_serve = down_train.astype(jnp.bfloat16)
    wide = tokens.astype(jnp.float32)
    scale = lax.rsqrt(lax.optimization_barrier(jnp.sum(wide * wide, axis=1)) / D + 1e-06)[:, None]
    gate = jnp.dot(tokens, gate_serve, preferred_element_type=jnp.float32)
    up_part = jnp.dot(tokens, up_serve, preferred_element_type=jnp.float32)
    hidden = (jax.nn.silu(gate * scale) * (up_part * scale)).astype(jnp.bfloat16)
    layer_out = jnp.dot(hidden, down_serve, preferred_element_type=jnp.float32).astype(jnp.bfloat16)
    return (gate_serve, up_serve, down_serve, layer_out)
```

```python
import functools

import jax
import jax.numpy as jnp
from jax import lax
from jax.experimental import pallas as pl
from jax.experimental.pallas import tpu as pltpu
from jax.sharding import PartitionSpec as P

MESH = pl.DeviceIdType.MESH
BF16 = jnp.bfloat16
F32 = jnp.float32
epsilon = 1e-06
CHUNKS = 4
X_ORDER = (0, 1, 2, 3)
Y_ORDER = (2, 3, 0, 1)
QUARTERS = 4
DUAL = (0, 1)
CHAIN = (2, 3)
scope = jax.named_scope


def flip(a, k):
    result = 0
    for bit in (1, 2, 4):
        own, other = (a // bit) % 2, (k // bit) % 2
        result = result + bit * (own + other - 2 * own * other)
    return result


def kernel(
    tok_in, gain_in, gate_in, up_in, down_in,
    wbuf, dbuf, layer_out,
    gain, w32, d32, dcast, xbuf, tbuf, acc, hidden, scale, keep, psend, precv, zsend, zrecv,
    load_g, load_t, load_w, load_d, tok_s, tok_r, own_s, fwd_s, w_r, dz_s, o_s, o_r, zr_s, d_s, d_r, p_s, p_r, z_s, z_r,
):
    f, t = lax.axis_index("fs"), lax.axis_index("tp")
    n_tp, n_fs = tbuf.shape[0], wbuf.shape[1]
    z, core = t // 2, t % 2
    fx, fy, fd = flip(f, 1), flip(f, 2), flip(f, 3)
    mate = flip(t, 1)
    rows = wbuf.shape[2]
    part = rows // CHUNKS
    w_ins = (gate_in, up_in)
    tall, width = dbuf.shape[1], dbuf.shape[2]
    quarter = tall // QUARTERS
    per = n_tp // n_fs
    n_tok = tbuf.shape[1]
    piece_rows = n_tok // n_tp
    n_z = n_tp // 2
    q = flip(f, z)
    side = jnp.logical_or(q == 1, q == 2)
    toward = fx + (fy - fx) * (q // 2)
    away = fy + (fx - fy) * (q // 2)

    def remote(src, dst, ss, rs, to_f, to_t):
        return pltpu.make_async_remote_copy(
            src_ref=src, dst_ref=dst, send_sem=ss, recv_sem=rs, device_id=(to_f, to_t), device_id_type=MESH
        )

    def load(w, i):
        return pltpu.make_async_copy(w_ins[w].at[pl.ds(i * part, part)], w32.at[w, pl.ds(i * part, part)], load_w.at[w, i])

    barrier = pltpu.get_barrier_semaphore()
    peers = [(fx, t), (fy, t)] + [(f, flip(t, k)) for k in range(1, n_tp)]
    for peer in peers:
        pl.semaphore_signal(barrier, inc=1, device_id=peer, device_id_type=MESH)

    load_gain = pltpu.make_async_copy(gain_in, gain, load_g)
    load_tok = pltpu.make_async_copy(tok_in, tbuf.at[t], load_t)
    load_down = [
        pltpu.make_async_copy(down_in.at[pl.ds(c * tall, tall)], d32.at[pl.ds(c * tall, tall)], load_d.at[c])
        for c in range(per)
    ]
    load_gain.start()
    for i in (0, 2):
        for w in range(2):
            load(w, i).start()
    load_tok.start()
    for copy in load_down:
        copy.start()
    for i in (1, 3):
        for w in range(2):
            load(w, i).start()

    def cast(w, i):
        block = pl.ds(i * part, part)
        load(w, i).wait()
        lanes = 128
        tall_gain = jnp.broadcast_to(gain[:, block], (lanes, part)).T
        for j in range(wbuf.shape[3] // lanes):
            columns = pl.ds(j * lanes, lanes)
            wbuf[w, f, block, columns] = (tall_gain * w32[w, block, columns]).astype(BF16)

    def tok_copy(src, piece, slot, to):
        return remote(src, tbuf.at[piece], tok_s.at[slot], tok_r.at[piece], f, to)

    def w_copy(w, src, i, sem, to):
        ref = wbuf.at[w, src, pl.ds(i * part, part)]
        return remote(ref, ref, sem, w_r.at[w, src, i], to, t)

    def send_own(step, w):
        w_copy(w, f, X_ORDER[step], own_s.at[0, w, X_ORDER[step]], fx).start()
        w_copy(w, f, Y_ORDER[step], own_s.at[1, w, Y_ORDER[step]], fy).start()

    def rows_of(h):
        return pl.ds(h * quarter, quarter)

    def dz_copy(c, h):
        return remote(dcast.at[c, rows_of(h)], dbuf.at[t, rows_of(h)], dz_s.at[c, h], d_r.at[t, h], f, f * per + c)

    def o_copy(slot, c, h, to):
        return remote(dcast.at[c, rows_of(h)], xbuf.at[slot, c, rows_of(h)], o_s.at[0, c, h], o_r.at[slot, c, h], to, t)

    def transit(c, h, to):
        ref = xbuf.at[2, c, rows_of(h)]
        return remote(ref, ref, o_s.at[1, c, h], o_r.at[2, c, h], to, t)

    def over_z(slot, c, h, column):
        return remote(
            xbuf.at[slot, c, rows_of(h)], dbuf.at[t, rows_of(h)], zr_s.at[slot, c, h], d_r.at[t, h], f, column * per + c
        )

    def d_copy(piece, h, to):
        ref = dbuf.at[piece, rows_of(h)]
        return remote(ref, ref, d_s.at[piece, h], d_r.at[piece, h], to, t)

    chain_stops = (q == 2, q == 1)
    chain_to = (fx + (fy - fx) * (q % 2) * (1 - q // 2), fy + (fx - fy) * (1 - q % 2) * (q // 2))

    def chain(k, h):
        piece = flip(t, k)

        @pl.when(jnp.logical_not(chain_stops[h % 2]))
        def _():
            if isinstance(k, int) and k == 0:
                @pl.when(q != 0)
                def _():
                    d_copy(piece, h, chain_to[h % 2]).wait_recv()
            else:
                d_copy(piece, h, chain_to[h % 2]).wait_recv()
            d_copy(piece, h, chain_to[h % 2]).start()

    def own_chain():
        for k in range(per):
            for h in range(QUARTERS):
                chain(k, h)

    def hand(k, h, to):
        piece = flip(t, k)
        d_copy(piece, h, to).wait_recv()
        d_copy(piece, h, to).start()

    load_gain.wait()
    cast(0, X_ORDER[0])
    cast(0, Y_ORDER[0])
    with scope("barrier"):
        pl.semaphore_wait(barrier, len(peers))
    cast(1, X_ORDER[0])
    cast(1, Y_ORDER[0])
    send_own(0, 0)
    load_tok.wait()
    for slot, k in enumerate((1, 2, 4, 6)):
        tok_copy(tbuf.at[t], t, slot, flip(t, k)).start()

    for c in range(per):
        load_down[c].wait()
        for h in range(QUARTERS):
            dcast[c, rows_of(h)] = d32[pl.ds(c * tall + h * quarter, quarter)].astype(BF16)

        @pl.when(t == f * per + c)
        def _():
            dbuf[t] = dcast[c]

        if c == 0:
            send_own(0, 1)

    @pl.when(side)
    def _():
        for h in DUAL:
            for c in range(per):
                o_copy(q - 1, c, h, toward).start()

    @pl.when(q == 3)
    def _():
        for c in range(per):
            o_copy(2, c, 0, fx).start()
            o_copy(2, c, 1, fy).start()

    for h in CHAIN + DUAL:
        for c in range(per):
            @pl.when(t != f * per + c)
            def _():
                dz_copy(c, h).start()

    @pl.when(q == 0)
    def _():
        own_chain()

    for w in range(2):
        cast(w, X_ORDER[1])
        cast(w, Y_ORDER[1])
        if w == 1:
            send_own(1, 0)
    send_own(1, 1)

    def arrive(step, w):
        i = X_ORDER[step]
        w_copy(w, fx, i, fwd_s.at[w, i], fy).wait_recv()
        i = Y_ORDER[step]
        w_copy(w, fy, i, fwd_s.at[w, i], fx).wait_recv()

    def forward(step, w):
        i = X_ORDER[step]
        w_copy(w, fx, i, fwd_s.at[w, i], fy).start()
        i = Y_ORDER[step]
        w_copy(w, fy, i, fwd_s.at[w, i], fx).start()

    def relay(way):
        h = 1 - way

        @pl.when(q == 1 + way)
        def _():
            for c in range(per):
                transit(c, h, toward).wait_recv()
                transit(c, h, toward).start()
                over_z(2, c, h, away).start()

    for w in range(2):
        with scope("arrive0"):
            arrive(0, w)
    with scope("transit"):
        relay(0)
        relay(1)
    for w in range(2):
        send_own(2, w)

    with scope("own_chain"):
        @pl.when(side)
        def _():
            own_chain()

    for w in range(2):
        send_own(3, w)

    with scope("over_z"):
        @pl.when(q == 0)
        def _():
            for h in DUAL:
                for c in range(per):
                    for slot, column in enumerate((fx, fy)):
                        o_copy(slot, c, h, fx).wait_recv()
                        over_z(slot, c, h, column).start()

    with scope("arrive1"):
        for w in range(2):
            forward(0, w)
        for w in range(2):
            arrive(1, w)
            forward(1, w)

    tile = 512

    def accumulate(src, first):
        def one(n, _):
            w, column = n // (wbuf.shape[3] // tile), pl.multiple_of(n % (wbuf.shape[3] // tile) * tile, tile)
            total = 0.0 if first else acc[w, :, pl.ds(column, tile)]
            for p in range(per):
                total = total + jnp.dot(
                    tbuf[src * per + p],
                    wbuf[w, src, pl.ds(p * width, width), pl.ds(column, tile)],
                    preferred_element_type=F32,
                )
            acc[w, :, pl.ds(column, tile)] = total
            return 0

        lax.fori_loop(0, 2 * (wbuf.shape[3] // tile), one, 0)

    with scope("over_z2"):
        @pl.when(q == 0)
        def _():
            for c in range(per):
                for h in DUAL:
                    o_copy(2, c, h, fx).wait_recv()
                    over_z(2, c, h, fd).start()

    with scope("tokens"):
        for slot, k in enumerate((2, 4, 6)):
            piece = flip(t, k)
            tok_copy(tbuf.at[piece], piece, 4 + slot, mate).wait_recv()
            tok_copy(tbuf.at[piece], piece, 4 + slot, mate).start()
        for k in (1, 3, 5, 7):
            tok_copy(tbuf.at[t], flip(t, k), 0, mate).wait_recv()

    with scope("own_chain3"):
        @pl.when(q == 3)
        def _():
            own_chain()

    def norm(i, _):
        block = pl.ds(i * piece_rows, piece_rows)
        squares = 0.0
        for p in range(n_tp):
            wide = tbuf[p, block].astype(F32)
            squares = squares + wide * wide
        scale[block] = lax.rsqrt(jnp.sum(squares, axis=1, keepdims=True) / (n_tp * width) + epsilon)
        return 0

    with scope("norm"):
        lax.fori_loop(0, n_tp, norm, 0)
    with scope("own_dot"):
        accumulate(f, True)
    with scope("arrive23"):
        for step in range(CHUNKS // 2, CHUNKS):
            for w in range(2):
                arrive(step, w)
    with scope("fx_dot"):
        accumulate(fx, False)
    with scope("fy_dot"):
        accumulate(fy, False)

    with scope("early"):
        @pl.when(q == 0)
        def _():
            for k in range(per, n_tp):
                for h in CHAIN:
                    chain(k, h)

        @pl.when(q == 1)
        def _():
            for k in (2, 3):
                for h in DUAL:
                    hand(k, h, fy)

        @pl.when(q == 2)
        def _():
            for k in (4, 5):
                for h in DUAL:
                    hand(k, h, fx)

        @pl.when(q == 3)
        def _():
            for k in (6, 7):
                hand(k, 0, fx)
                hand(k, 1, fy)

    with scope("fd_wait"):
        for i in (0, 2, 1, 3):
            for w in range(2):
                w_copy(w, fd, i, fwd_s.at[w, i], fx).wait_recv()
    with scope("fd_dot"):
        accumulate(fd, False)

    with scope("late"):
        @pl.when(q == 0)
        def _():
            for j in range(2):
                for h in DUAL:
                    hand(2 + j, h, fy)
                    hand(4 + j, h, fx)

    def make_hidden(n, _):
        columns = pl.ds(pl.multiple_of(n * tile, tile), tile)
        s = scale[...]
        g = acc[0, :, columns] * s
        hidden[:, columns] = (g / (1.0 + jnp.exp(-g)) * (acc[1, :, columns] * s)).astype(BF16)
        return 0

    with scope("hidden"):
        lax.fori_loop(0, hidden.shape[1] // tile, make_hidden, 0)

    def p_copy(k):
        return remote(psend.at[k], precv.at[k], p_s.at[k], p_r.at[k], f, mate)

    def z_copy(k, dz, piece):
        to = flip(t, 2 * dz)
        return remote(zsend.at[k, to // 2], zrecv.at[z, piece], z_s.at[k, dz], z_r.at[z, piece], f, to)

    def z_arrival(dz, piece):
        src = flip(t, 2 * dz)
        return remote(zsend.at[0, 0], zrecv.at[src // 2, piece], z_s.at[0, dz], z_r.at[src // 2, piece], f, src)

    def finish(k):
        p_copy(k).wait_recv()
        for b in range(n_z):
            block = (keep[flip(k, 1), b] + precv[k, b].astype(F32)).astype(BF16)
            zsend[k, b] = block
        piece = flip(mate, k)
        zrecv[z, piece] = zsend[k, z]
        for dz in range(1, n_z):
            z_copy(k, dz, piece).start()

    def product(k):
        piece = flip(t, k)
        out = jnp.dot(hidden[...], dbuf[piece], preferred_element_type=F32)
        out = out.reshape(n_z, 2, piece_rows, width)

        @pl.when(core == 0)
        def _():
            keep[k] = out[:, 0]
            psend[k] = out[:, 1].astype(BF16)

        @pl.when(core == 1)
        def _():
            keep[k] = out[:, 1]
            psend[k] = out[:, 0].astype(BF16)

        p_copy(k).start()

    def take(k):
        piece = flip(t, k)
        r = k // 2
        passed = jnp.logical_or(
            jnp.logical_or(jnp.logical_and(r == 1, q < 2), jnp.logical_and(r == 2, q % 2 == 0)),
            jnp.logical_and(r == 3, q == 3),
        )

        @pl.when(jnp.logical_and(r > 0, jnp.logical_not(passed)))
        def _():
            for h in DUAL:
                d_copy(piece, h, fx).wait_recv()

        for side_h in range(2):
            @pl.when(chain_stops[side_h])
            def _():
                d_copy(piece, CHAIN[side_h], fx).wait_recv()

                @pl.when(r == 0)
                def _():
                    d_copy(piece, DUAL[side_h], fx).wait_recv()

    def turn(i):
        j = i // 2
        one, two, three = [jnp.where(j == n, 1, 0) for n in (1, 2, 3)]
        first, second = jnp.where(q == 1, 1, 0), jnp.where(q == 2, 1, 0)
        return i + 2 * (first * (two - three) + second * (one + two - 2 * three))

    def step(i, _):
        @pl.when(jnp.logical_and(i % 2 == 0, i >= 2))
        def _():
            with scope("finish"):
                finish(turn(i - 2))
                finish(turn(i - 1))

        with scope("pass_on"):
            for role, lead in ((q == 3, 1), (side, 3)):
                @pl.when(jnp.logical_and(role, i == 2))
                def _():
                    for n in range(lead):
                        for h in CHAIN:
                            chain(i + n, h)

                @pl.when(jnp.logical_and(role, jnp.logical_and(i >= 2, i + lead < n_tp)))
                def _():
                    for h in CHAIN:
                        chain(i + lead, h)

        @pl.when(i < n_tp)
        def _():
            with scope("take"):
                take(turn(i))
            with scope("product"):
                product(turn(i))

        @pl.when(i == n_tp // 2)
        def _():
            with scope("sent"):
                for slot in range(4):
                    tok_copy(tbuf.at[t], t, slot, mate).wait_send()
                for slot in range(3):
                    tok_copy(tbuf.at[t], t, 4 + slot, mate).wait_send()
                for w in range(2):
                    for n in range(CHUNKS):
                        w_copy(w, f, n, own_s.at[0, w, n], fx).wait_send()
                        w_copy(w, f, n, own_s.at[1, w, n], fy).wait_send()
                        w_copy(w, f, n, fwd_s.at[w, n], fx).wait_send()
                for c in range(per):
                    for h in range(QUARTERS):
                        @pl.when(t != f * per + c)
                        def _():
                            dz_copy(c, h).wait_send()

                @pl.when(q != 0)
                def _():
                    for c in range(per):
                        for h in DUAL:
                            o_copy(2, c, h, fx).wait_send()

                @pl.when(q == 0)
                def _():
                    for slot in range(3):
                        for c in range(per):
                            for h in DUAL:
                                over_z(slot, c, h, f).wait_send()

                for way in range(2):
                    @pl.when(q == 1 + way)
                    def _():
                        for c in range(per):
                            transit(c, 1 - way, toward).wait_send()
                            over_z(2, c, 1 - way, away).wait_send()

        return 0

    lax.fori_loop(0, n_tp + 1, step, 0)

    with scope("sent2"):
        for k in range(n_tp):
            piece = flip(t, k)
            for h in range(QUARTERS):
                if k < per or h in CHAIN:
                    go = jnp.logical_not(chain_stops[h % 2])
                else:
                    go = (None, q < 2, q % 2 == 0, q == 3)[k // 2]

                @pl.when(go)
                def _():
                    d_copy(piece, h, fx).wait_send()
            p_copy(k).wait_send()

    for piece in range(n_tp):
        with scope("z_wait"):
            for dz in range(1, n_z):
                z_arrival(dz, piece).wait_recv()
        total = zrecv[0, piece].astype(F32)
        for b in range(1, n_z):
            total = total + zrecv[b, piece].astype(F32)
        layer_out[:, pl.ds(piece * width, width)] = total.astype(BF16)
    with scope("sent3"):
        for k in range(n_tp):
            for dz in range(1, n_z):
                z_copy(k, dz, k).wait_send()


def write_out(weights, down, layer, gate_out, up_out, down_out, layer_out, w_s, d_s, l_s):
    _, n_fs, rows, _ = weights.shape
    n_tp, _, width = down.shape
    copies = [pltpu.make_async_copy(layer, layer_out, l_s)]
    for w, out in enumerate((gate_out, up_out)):
        for src in range(n_fs):
            copies.append(pltpu.make_async_copy(weights.at[w, src], out.at[pl.ds(src * rows, rows)], w_s.at[w, src]))
    for j in range(n_tp):
        copies.append(pltpu.make_async_copy(down.at[j], down_out.at[:, pl.ds(j * width, width)], d_s.at[j]))
    for copy in copies:
        copy.start()
    for copy in copies:
        copy.wait()


def body(tokens, norm_gain, gate_train, up_train, down_train, *, n_fs, n_tp):
    n_tok, width = tokens.shape
    rows, cols = gate_train.shape
    tall = down_train.shape[0] * n_fs // n_tp
    piece_rows = n_tok // n_tp
    n_z = n_tp // 2
    hbm = pl.BlockSpec(memory_space=pltpu.HBM)
    vmem = pl.BlockSpec(memory_space=pltpu.VMEM)
    dma = pltpu.SemaphoreType.DMA
    weights, down, layer = pl.pallas_call(
        kernel,
        out_shape=(
            pltpu.VMEM((2, n_fs, rows, cols), BF16),
            pltpu.VMEM((n_tp, tall, width), BF16),
            pltpu.VMEM((piece_rows, width * n_tp), BF16),
        ),
        in_specs=[hbm] * 5,
        out_specs=(vmem, vmem, vmem),
        scratch_shapes=[
            pltpu.VMEM((1, rows), F32),
            pltpu.VMEM((2, rows, cols), F32),
            pltpu.VMEM(down_train.shape, F32),
            pltpu.VMEM((n_tp // n_fs, tall, width), BF16),
            pltpu.VMEM((3, n_tp // n_fs, tall // QUARTERS * len(DUAL), width), BF16),
            pltpu.VMEM((n_tp, n_tok, width), BF16),
            pltpu.VMEM((2, n_tok, cols), F32),
            pltpu.VMEM((n_tok, cols), BF16),
            pltpu.VMEM((n_tok, 1), F32),
            pltpu.VMEM((n_tp, n_z, piece_rows, width), F32),
            pltpu.VMEM((n_tp, n_z, piece_rows, width), BF16),
            pltpu.VMEM((n_tp, n_z, piece_rows, width), BF16),
            pltpu.VMEM((n_tp, n_z, piece_rows, width), BF16),
            pltpu.VMEM((n_z, n_tp, piece_rows, width), BF16),
            dma,
            dma,
            dma((2, CHUNKS)),
            dma((n_tp // n_fs,)),
            dma((7,)),
            dma((n_tp,)),
            dma((2, 2, CHUNKS)),
            dma((2, CHUNKS)),
            dma((2, n_fs, CHUNKS)),
            dma((n_tp // n_fs, QUARTERS)),
            dma((2, n_tp // n_fs, len(DUAL))),
            dma((3, n_tp // n_fs, len(DUAL))),
            dma((3, n_tp // n_fs, len(DUAL))),
            dma((n_tp, QUARTERS)),
            dma((n_tp, QUARTERS)),
            dma((n_tp,)),
            dma((n_tp,)),
            dma((n_tp, n_z)),
            dma((n_z, n_tp)),
        ],
        compiler_params=pltpu.CompilerParams(
            collective_id=0, has_side_effects=True, vmem_limit_bytes=51 * 1024 * 1024
        ),
    )(tokens, norm_gain[None, :], gate_train, up_train, down_train)
    return pl.pallas_call(
        write_out,
        out_shape=(
            jax.ShapeDtypeStruct((rows * n_fs, cols), BF16),
            jax.ShapeDtypeStruct((rows * n_fs, cols), BF16),
            jax.ShapeDtypeStruct((tall, width * n_tp), BF16),
            jax.ShapeDtypeStruct((piece_rows, width * n_tp), BF16),
        ),
        in_specs=[vmem] * 3,
        out_specs=(pl.BlockSpec(memory_space=pl.ANY),) * 4,
        scratch_shapes=[dma((2, n_fs)), dma((n_tp,)), dma],
        compiler_params=pltpu.CompilerParams(vmem_limit_bytes=4 * 1024 * 1024),
    )(weights, down, layer)


def plain(tokens, norm_gain, gate_train, up_train, down_train):
    gate_local = (norm_gain[:, None] * gate_train).astype(BF16)
    up_local = (norm_gain[:, None] * up_train).astype(BF16)
    down_local = down_train.astype(BF16)
    features = lax.all_gather(tokens, "tp", axis=1, tiled=True)
    wide = features.astype(F32)
    squares = jnp.sum(wide * wide, axis=1)
    gate_whole = lax.all_gather(gate_local, "fs", axis=0, tiled=True)
    up_whole = lax.all_gather(up_local, "fs", axis=0, tiled=True)
    gate_sum = jnp.dot(features, gate_whole, preferred_element_type=F32)
    up_sum = jnp.dot(features, up_whole, preferred_element_type=F32)
    down_rows = lax.all_gather(down_local, "fs", axis=0, tiled=True)
    down_whole = lax.all_to_all(down_rows, "tp", split_axis=0, concat_axis=1, tiled=True)
    scale = lax.rsqrt(squares / features.shape[1] + epsilon)[:, None]
    hidden = (jax.nn.silu(gate_sum * scale) * (up_sum * scale)).astype(BF16)
    mixed = lax.psum_scatter(
        jnp.dot(hidden, down_whole, preferred_element_type=F32).astype(BF16), "tp", scatter_dimension=0, tiled=True
    )
    return (gate_whole, up_whole, down_whole, mixed)


def solution(mesh):
    n_fs, n_tp = mesh.shape["fs"], mesh.shape["tp"]
    fast = n_fs == 4 and n_tp == 8
    return jax.shard_map(
        functools.partial(body, n_fs=n_fs, n_tp=n_tp) if fast else plain,
        mesh=mesh,
        in_specs=(P("fs", "tp"), P("fs"), P("fs", "tp"), P("fs", "tp"), P("fs", "tp")),
        out_specs=(P(None, "tp"), P(None, "tp"), P("tp", None), P(("fs", "tp"), None)),
        check_vma=False,
    )
```

```python
import functools

import jax
import jax.numpy as jnp
from jax import lax
from jax.experimental import pallas as pl
from jax.experimental.pallas import tpu as pltpu
from jax.sharding import PartitionSpec as P

MESH = pl.DeviceIdType.MESH
BF16 = jnp.bfloat16
F32 = jnp.float32
epsilon = 1e-06
CHUNKS = 4
X_ORDER = (0, 1, 2, 3)
Y_ORDER = (2, 3, 0, 1)
QUARTERS = 4
DUAL = (0, 1)
CHAIN = (2, 3)
scope = jax.named_scope


def flip(a, k):
    result = 0
    for bit in (1, 2, 4):
        own, other = (a // bit) % 2, (k // bit) % 2
        result = result + bit * (own + other - 2 * own * other)
    return result


def kernel(
    tok_in, gain_in, gate_in, up_in, down_in,
    wbuf, dbuf, layer_out,
    gain, w32, d32, dcast, xbuf, tbuf, acc, hidden, scale, keep, psend, precv, zsend, zrecv,
    load_g, load_t, load_w, load_d, tok_s, tok_r, w_s, w_r, dz_s, o_s, o_r, zr_s, d_s, d_r, p_s, p_r, z_s, z_r,
):
    f, t = lax.axis_index("fs"), lax.axis_index("tp")
    n_tp, n_fs = tbuf.shape[0], wbuf.shape[1]
    z, core = t // 2, t % 2
    fx, fy, fd = flip(f, 1), flip(f, 2), flip(f, 3)
    mate = flip(t, 1)
    base = t - core
    rows = wbuf.shape[2]
    part = rows // CHUNKS
    w_ins = (gate_in, up_in)
    tall, width = dbuf.shape[1], dbuf.shape[2]
    quarter = tall // QUARTERS
    per = n_tp // n_fs
    n_tok = tbuf.shape[1]
    piece_rows = n_tok // n_tp
    n_z = n_tp // 2
    q = flip(f, z)
    side = jnp.logical_or(q == 1, q == 2)
    toward = fx + (fy - fx) * (q // 2)
    away = fy + (fx - fy) * (q // 2)

    def remote(src, dst, ss, rs, to_f, to_t):
        return pltpu.make_async_remote_copy(
            src_ref=src, dst_ref=dst, send_sem=ss, recv_sem=rs, device_id=(to_f, to_t), device_id_type=MESH
        )

    def load(w, i):
        return pltpu.make_async_copy(w_ins[w].at[pl.ds(i * part, part)], w32.at[w, pl.ds(i * part, part)], load_w.at[w, i])

    barrier = pltpu.get_barrier_semaphore()
    peers = [(fx, t), (fy, t)] + [(f, flip(t, k)) for k in range(1, n_tp)]
    for peer in peers:
        pl.semaphore_signal(barrier, inc=1, device_id=peer, device_id_type=MESH)

    load_gain = pltpu.make_async_copy(gain_in, gain, load_g)
    load_tok = pltpu.make_async_copy(tok_in, tbuf.at[t], load_t)
    load_down = [
        pltpu.make_async_copy(down_in.at[pl.ds(c * tall, tall)], d32.at[pl.ds(c * tall, tall)], load_d.at[c])
        for c in range(per)
    ]
    load_gain.start()
    for i in (0, 2):
        for w in range(2):
            load(w, i).start()
    load_tok.start()
    for copy in load_down:
        copy.start()
    for i in (1, 3):
        for w in range(2):
            load(w, i).start()

    def cast(w, i):
        block = pl.ds(i * part, part)
        load(w, i).wait()
        lanes = 128
        tall_gain = jnp.broadcast_to(gain[:, block], (lanes, part)).T
        for j in range(wbuf.shape[3] // lanes):
            columns = pl.ds(j * lanes, lanes)
            wbuf[w, f, block, columns] = (tall_gain * w32[w, block, columns]).astype(BF16)

    def tok_copy(piece, dz, to):
        return remote(tbuf.at[piece], tbuf.at[piece], tok_s, tok_r.at[dz], f, to)

    def w_copy(src, i, to):
        ref = wbuf.at[:, src, pl.ds(i * part, part)]
        return remote(ref, ref, w_s, w_r.at[src, i], to, t)

    def send_own(step):
        w_copy(f, X_ORDER[step], fx).start()
        w_copy(f, Y_ORDER[step], fy).start()

    def rows_of(h):
        return pl.ds(h * quarter, quarter)

    def dz_copy(c, h):
        return remote(dcast.at[c, rows_of(h)], dbuf.at[t, rows_of(h)], dz_s, d_r.at[t, h], f, f * per + c)

    def o_copy(slot, h, to):
        return remote(dcast.at[:, rows_of(h)], xbuf.at[slot, :, rows_of(h)], o_s, o_r.at[slot, h], to, t)

    def transit(h, to):
        ref = xbuf.at[2, :, rows_of(h)]
        return remote(ref, ref, o_s, o_r.at[2, h], to, t)

    def over_z(slot, c, h, column):
        return remote(xbuf.at[slot, c, rows_of(h)], dbuf.at[t, rows_of(h)], zr_s, d_r.at[t, h], f, column * per + c)

    def d_copy(piece, h, to):
        ref = dbuf.at[piece, rows_of(h)]
        return remote(ref, ref, d_s, d_r.at[piece, h], to, t)

    def sent(ref, sem):
        remote(ref, ref, sem, sem, fx, t).wait_send()

    chain_stops = (q == 2, q == 1)
    chain_to = (fx + (fy - fx) * (q % 2) * (1 - q // 2), fy + (fx - fy) * (1 - q % 2) * (q // 2))

    def chain(k, hs):
        piece = flip(base, k)
        for h in hs:
            @pl.when(jnp.logical_not(chain_stops[h % 2]))
            def _():
                if isinstance(k, int) and k < per:
                    @pl.when(jnp.logical_or(q != 0, core != k))
                    def _():
                        d_copy(piece, h, chain_to[h % 2]).wait_recv()
                else:
                    d_copy(piece, h, chain_to[h % 2]).wait_recv()
                d_copy(piece, h, chain_to[h % 2]).start()

    inner = jnp.logical_or(z == 1, z == 2)

    def chain_next(n):
        r = n // 2
        chain(2 * jnp.where(inner, 1 + r, 3 - r) + n % 2, CHAIN)

    def own_chain():
        for k in range(per):
            chain(k, range(QUARTERS))

    def hand(k, h, to):
        piece = flip(base, k)
        d_copy(piece, h, to).wait_recv()
        d_copy(piece, h, to).start()

    load_gain.wait()
    cast(0, X_ORDER[0])
    cast(0, Y_ORDER[0])
    cast(1, X_ORDER[0])
    cast(1, Y_ORDER[0])
    with scope("barrier"):
        pl.semaphore_wait(barrier, len(peers))
    send_own(0)
    load_tok.wait()
    for dz, k in enumerate((1, 2, 4, 6)):
        tok_copy(t, dz, flip(t, k)).start()

    for c in range(per):
        load_down[c].wait()
        for h in range(QUARTERS):
            dcast[c, rows_of(h)] = d32[pl.ds(c * tall + h * quarter, quarter)].astype(BF16)

        @pl.when(t == f * per + c)
        def _():
            dbuf[t] = dcast[c]

    cast(0, X_ORDER[1])
    cast(0, Y_ORDER[1])

    @pl.when(side)
    def _():
        for h in DUAL:
            o_copy(q - 1, h, toward).start()

    @pl.when(q == 3)
    def _():
        o_copy(2, 0, fx).start()
        o_copy(2, 1, fy).start()

    for h in CHAIN + DUAL:
        for c in range(per):
            @pl.when(t != f * per + c)
            def _():
                dz_copy(c, h).start()

    cast(1, X_ORDER[1])
    cast(1, Y_ORDER[1])

    @pl.when(q == 0)
    def _():
        own_chain()

    send_own(1)

    def arrive(step):
        w_copy(fx, X_ORDER[step], fy).wait_recv()
        w_copy(fy, Y_ORDER[step], fx).wait_recv()

    def forward(step):
        w_copy(fx, X_ORDER[step], fy).start()
        w_copy(fy, Y_ORDER[step], fx).start()

    with scope("arrive0"):
        arrive(0)
    with scope("transit"):
        for way in range(2):
            @pl.when(q == 1 + way)
            def _():
                transit(1 - way, toward).wait_recv()
                transit(1 - way, toward).start()
                for c in range(per):
                    over_z(2, c, 1 - way, away).start()

    send_own(2)

    with scope("own_chain"):
        @pl.when(side)
        def _():
            own_chain()

    send_own(3)

    with scope("over_z"):
        @pl.when(q == 0)
        def _():
            for h in DUAL:
                for slot, column in enumerate((fx, fy)):
                    o_copy(slot, h, fx).wait_recv()
                    for c in range(per):
                        over_z(slot, c, h, column).start()

    with scope("arrive1"):
        forward(0)
        arrive(1)

    with scope("over_z2"):
        @pl.when(q == 0)
        def _():
            for h in DUAL:
                o_copy(2, h, fx).wait_recv()
                for c in range(per):
                    over_z(2, c, h, fd).start()

    with scope("chain0"):
        @pl.when(q == 0)
        def _():
            chain_next(0)
            chain_next(1)

    forward(1)

    tile = 512

    def accumulate(src, first):
        def one(n, _):
            w, column = n // (wbuf.shape[3] // tile), pl.multiple_of(n % (wbuf.shape[3] // tile) * tile, tile)
            total = 0.0 if first else acc[w, :, pl.ds(column, tile)]
            for p in range(per):
                total = total + jnp.dot(
                    tbuf[src * per + p],
                    wbuf[w, src, pl.ds(p * width, width), pl.ds(column, tile)],
                    preferred_element_type=F32,
                )
            acc[w, :, pl.ds(column, tile)] = total
            return 0

        lax.fori_loop(0, 2 * (wbuf.shape[3] // tile), one, 0)

    with scope("tokens"):
        for dz in range(1, n_z):
            piece = flip(t, 2 * dz)
            tok_copy(piece, dz, mate).wait_recv()
            tok_copy(piece, 0, mate).start()
        remote(tbuf.at[pl.ds(0, n_z)], tbuf.at[pl.ds(0, n_z)], tok_s, tok_r.at[0], f, mate).wait_recv()

    with scope("own_chain3"):
        @pl.when(q == 3)
        def _():
            own_chain()

    def norm(i, _):
        block = pl.ds(i * piece_rows, piece_rows)
        squares = 0.0
        for p in range(n_tp):
            wide = tbuf[p, block].astype(F32)
            squares = squares + wide * wide
        scale[block] = lax.rsqrt(jnp.sum(squares, axis=1, keepdims=True) / (n_tp * width) + epsilon)
        return 0

    with scope("norm"):
        lax.fori_loop(0, n_tp, norm, 0)
    with scope("own_dot"):
        accumulate(f, True)
    with scope("arrive23"):
        for step in range(CHUNKS // 2, CHUNKS):
            arrive(step)
    with scope("fx_dot"):
        accumulate(fx, False)
    with scope("fy_dot"):
        accumulate(fy, False)

    with scope("early"):
        @pl.when(q == 0)
        def _():
            for n in range(2, 6):
                chain_next(n)

        for place, k, to in ((1, 2, fy), (2, 4, fx)):
            @pl.when(q == place)
            def _():
                chain_next(0)
                chain_next(1)
                for h in DUAL:
                    hand(k, h, to)
                    d_copy(flip(base, k + 1), h, to).wait_recv()

        @pl.when(q == 3)
        def _():
            hand(6, 0, fx)
            hand(6, 1, fy)

    with scope("fd_wait"):
        for i in range(CHUNKS):
            w_copy(fd, i, fx).wait_recv()
    with scope("fd_dot"):
        accumulate(fd, False)

    with scope("late"):
        @pl.when(q == 0)
        def _():
            for j in range(2):
                for h in DUAL:
                    hand(2 + j, h, fy)
                    hand(4 + j, h, fx)

    def make_hidden(n, _):
        columns = pl.ds(pl.multiple_of(n * tile, tile), tile)
        s = scale[...]
        g = acc[0, :, columns] * s
        hidden[:, columns] = (g / (1.0 + jnp.exp(-g)) * (acc[1, :, columns] * s)).astype(BF16)
        return 0

    with scope("hidden"):
        lax.fori_loop(0, hidden.shape[1] // tile, make_hidden, 0)

    def p_copy(k):
        return remote(psend.at[k], precv.at[k], p_s, p_r.at[k], f, mate)

    def z_copy(k, dz, piece):
        to = flip(t, 2 * dz)
        return remote(zsend.at[k, to // 2], zrecv.at[z, piece], z_s, z_r.at[piece], f, to)

    def finish(k):
        p_copy(k).wait_recv()
        for b in range(n_z):
            zsend[k, b] = (keep[k, b] + precv[k, b].astype(F32)).astype(BF16)
        piece = flip(base, k)
        zrecv[z, piece] = zsend[k, z]
        for dz in range(1, n_z):
            z_copy(k, dz, piece).start()

    def product(k):
        piece = flip(base, k)
        out = jnp.dot(hidden[...], dbuf[piece], preferred_element_type=F32)
        out = out.reshape(n_z, 2, piece_rows, width)

        @pl.when(core == 0)
        def _():
            keep[k] = out[:, 0]
            psend[k] = out[:, 1].astype(BF16)

        @pl.when(core == 1)
        def _():
            keep[k] = out[:, 1]
            psend[k] = out[:, 0].astype(BF16)

        p_copy(k).start()

    def take(k):
        piece = flip(base, k)
        r = k // 2
        passed = jnp.logical_or(
            jnp.logical_or(jnp.logical_and(r == 1, q < 2), jnp.logical_and(r == 2, q % 2 == 0)),
            jnp.logical_and(r == 3, q == 3),
        )

        @pl.when(jnp.logical_and(r > 0, jnp.logical_not(passed)))
        def _():
            for h in DUAL:
                d_copy(piece, h, fx).wait_recv()

        for side_h in range(2):
            @pl.when(chain_stops[side_h])
            def _():
                d_copy(piece, CHAIN[side_h], fx).wait_recv()

                @pl.when(r == 0)
                def _():
                    d_copy(piece, DUAL[side_h], fx).wait_recv()

    def turn(i):
        k = i
        for here, order in (
            (jnp.logical_and(inner, q == 2), (0, 1, 4, 2, 5, 6, 3, 7)),
            (jnp.logical_and(inner, q == 3), (0, 1, 2, 4, 6, 7, 3, 5)),
            (jnp.logical_and(jnp.logical_not(inner), q % 2 == 0), (0, 1, 6, 7, 4, 5, 2, 3)),
            (jnp.logical_and(jnp.logical_not(inner), q % 2 == 1), (0, 1, 6, 7, 4, 2, 5, 3)),
        ):
            mine = 0
            for n, v in enumerate(order):
                mine = mine + v * jnp.where(i == n, 1, 0)
            k = jnp.where(here, mine, k)
        return k

    def pass_on(i):
        @pl.when(jnp.logical_and(side, i == 2))
        def _():
            chain_next(i)

        @pl.when(jnp.logical_and(side, jnp.logical_and(i >= 2, i <= 4)))
        def _():
            chain_next(i + 1)

        for place, k, to in ((1, 3, fy), (2, 5, fx)):
            @pl.when(jnp.logical_and(q == place, i == 4))
            def _():
                for h in DUAL:
                    d_copy(flip(base, k), h, to).start()

        @pl.when(jnp.logical_and(q == 3, i == 2))
        def _():
            chain_next(i - 2)
            chain_next(i - 1)
            hand(7, 0, fx)
            hand(7, 1, fy)

        @pl.when(jnp.logical_and(q == 3, jnp.logical_and(i >= 3, i <= 4)))
        def _():
            chain_next(i - 1)

        @pl.when(jnp.logical_and(q == 3, jnp.logical_and(i >= 4, i <= 5)))
        def _():
            chain_next(i)

    def step(i, _):
        with scope("pass_on"):
            pass_on(i)

        @pl.when(i >= 1)
        def _():
            with scope("finish"):
                finish(turn(i - 1))

        @pl.when(i < n_tp)
        def _():
            k = turn(i)
            with scope("take"):
                take(k)
            with scope("product"):
                product(k)

        return 0

    lax.fori_loop(0, n_tp + 1, step, 0)

    with scope("sent"):
        sent(tbuf.at[pl.ds(0, n_tp - 1)], tok_s)
        sent(wbuf.at[:, pl.ds(0, n_fs - 1)], w_s)
        sent(psend, p_s)

        @pl.when(q == 0)
        def _():
            sent(dcast.at[0], dz_s)
            sent(xbuf, zr_s)
            sent(dbuf.at[pl.ds(0, 7)], d_s)

        @pl.when(side)
        def _():
            sent(xbuf.at[:, :, rows_of(0)], o_s)
            sent(xbuf.at[0, 0], zr_s)
            sent(dbuf.at[pl.ds(0, 7), pl.ds(0, 2 * quarter)], d_s)

        @pl.when(q == 3)
        def _():
            sent(xbuf.at[0], o_s)
            sent(dbuf.at[pl.ds(0, 6)], d_s)

        @pl.when(q != 0)
        def _():
            sent(dcast, dz_s)

    for piece in range(n_tp):
        with scope("z_wait"):
            others = zrecv.at[pl.ds(0, n_z - 1), piece]
            remote(others, others, z_s, z_r.at[piece], f, mate).wait_recv()
        total = zrecv[0, piece].astype(F32)
        for b in range(1, n_z):
            total = total + zrecv[b, piece].astype(F32)
        layer_out[:, pl.ds(piece * width, width)] = total.astype(BF16)
    sent(zsend.at[:, pl.ds(0, n_z - 1)], z_s)


def write_out(weights, down, layer, gate_out, up_out, down_out, layer_out, w_s, d_s, l_s):
    _, n_fs, rows, _ = weights.shape
    n_tp, _, width = down.shape
    copies = [pltpu.make_async_copy(layer, layer_out, l_s)]
    for w, out in enumerate((gate_out, up_out)):
        for src in range(n_fs):
            copies.append(pltpu.make_async_copy(weights.at[w, src], out.at[pl.ds(src * rows, rows)], w_s.at[w, src]))
    for j in range(n_tp):
        copies.append(pltpu.make_async_copy(down.at[j], down_out.at[:, pl.ds(j * width, width)], d_s.at[j]))
    for copy in copies:
        copy.start()
    for copy in copies:
        copy.wait()


def body(tokens, norm_gain, gate_train, up_train, down_train, *, n_fs, n_tp):
    n_tok, width = tokens.shape
    rows, cols = gate_train.shape
    tall = down_train.shape[0] * n_fs // n_tp
    piece_rows = n_tok // n_tp
    n_z = n_tp // 2
    hbm = pl.BlockSpec(memory_space=pltpu.HBM)
    vmem = pl.BlockSpec(memory_space=pltpu.VMEM)
    dma = pltpu.SemaphoreType.DMA
    weights, down, layer = pl.pallas_call(
        kernel,
        out_shape=(
            pltpu.VMEM((2, n_fs, rows, cols), BF16),
            pltpu.VMEM((n_tp, tall, width), BF16),
            pltpu.VMEM((piece_rows, width * n_tp), BF16),
        ),
        in_specs=[hbm] * 5,
        out_specs=(vmem, vmem, vmem),
        scratch_shapes=[
            pltpu.VMEM((1, rows), F32),
            pltpu.VMEM((2, rows, cols), F32),
            pltpu.VMEM(down_train.shape, F32),
            pltpu.VMEM((n_tp // n_fs, tall, width), BF16),
            pltpu.VMEM((3, n_tp // n_fs, tall // QUARTERS * len(DUAL), width), BF16),
            pltpu.VMEM((n_tp, n_tok, width), BF16),
            pltpu.VMEM((2, n_tok, cols), F32),
            pltpu.VMEM((n_tok, cols), BF16),
            pltpu.VMEM((n_tok, 1), F32),
            pltpu.VMEM((n_tp, n_z, piece_rows, width), F32),
            pltpu.VMEM((n_tp, n_z, piece_rows, width), BF16),
            pltpu.VMEM((n_tp, n_z, piece_rows, width), BF16),
            pltpu.VMEM((n_tp, n_z, piece_rows, width), BF16),
            pltpu.VMEM((n_z, n_tp, piece_rows, width), BF16),
            dma,
            dma,
            dma((2, CHUNKS)),
            dma((n_tp // n_fs,)),
            dma,
            dma((n_z,)),
            dma,
            dma((n_fs, CHUNKS)),
            dma,
            dma,
            dma((3, len(DUAL))),
            dma,
            dma,
            dma((n_tp, QUARTERS)),
            dma,
            dma((n_tp,)),
            dma,
            dma((n_tp,)),
        ],
        compiler_params=pltpu.CompilerParams(
            collective_id=0, has_side_effects=True, vmem_limit_bytes=51 * 1024 * 1024
        ),
    )(tokens, norm_gain[None, :], gate_train, up_train, down_train)
    return pl.pallas_call(
        write_out,
        out_shape=(
            jax.ShapeDtypeStruct((rows * n_fs, cols), BF16),
            jax.ShapeDtypeStruct((rows * n_fs, cols), BF16),
            jax.ShapeDtypeStruct((tall, width * n_tp), BF16),
            jax.ShapeDtypeStruct((piece_rows, width * n_tp), BF16),
        ),
        in_specs=[vmem] * 3,
        out_specs=(pl.BlockSpec(memory_space=pl.ANY),) * 4,
        scratch_shapes=[dma((2, n_fs)), dma((n_tp,)), dma],
        compiler_params=pltpu.CompilerParams(vmem_limit_bytes=4 * 1024 * 1024),
    )(weights, down, layer)


def plain(tokens, norm_gain, gate_train, up_train, down_train):
    gate_local = (norm_gain[:, None] * gate_train).astype(BF16)
    up_local = (norm_gain[:, None] * up_train).astype(BF16)
    down_local = down_train.astype(BF16)
    features = lax.all_gather(tokens, "tp", axis=1, tiled=True)
    wide = features.astype(F32)
    squares = jnp.sum(wide * wide, axis=1)
    gate_whole = lax.all_gather(gate_local, "fs", axis=0, tiled=True)
    up_whole = lax.all_gather(up_local, "fs", axis=0, tiled=True)
    gate_sum = jnp.dot(features, gate_whole, preferred_element_type=F32)
    up_sum = jnp.dot(features, up_whole, preferred_element_type=F32)
    down_rows = lax.all_gather(down_local, "fs", axis=0, tiled=True)
    down_whole = lax.all_to_all(down_rows, "tp", split_axis=0, concat_axis=1, tiled=True)
    scale = lax.rsqrt(squares / features.shape[1] + epsilon)[:, None]
    hidden = (jax.nn.silu(gate_sum * scale) * (up_sum * scale)).astype(BF16)
    mixed = lax.psum_scatter(
        jnp.dot(hidden, down_whole, preferred_element_type=F32).astype(BF16), "tp", scatter_dimension=0, tiled=True
    )
    return (gate_whole, up_whole, down_whole, mixed)


def solution(mesh):
    n_fs, n_tp = mesh.shape["fs"], mesh.shape["tp"]
    fast = n_fs == 4 and n_tp == 8
    return jax.shard_map(
        functools.partial(body, n_fs=n_fs, n_tp=n_tp) if fast else plain,
        mesh=mesh,
        in_specs=(P("fs", "tp"), P("fs"), P("fs", "tp"), P("fs", "tp"), P("fs", "tp")),
        out_specs=(P(None, "tp"), P(None, "tp"), P("tp", None), P(("fs", "tp"), None)),
        check_vma=False,
    )
```

```python
import functools

import jax
import jax.numpy as jnp
from jax import lax
from jax.experimental import pallas as pl
from jax.experimental.pallas import tpu as pltpu
from jax.sharding import PartitionSpec as P

MESH = pl.DeviceIdType.MESH
BF16 = jnp.bfloat16
F32 = jnp.float32
epsilon = 1e-06
CHUNKS = 4
X_ORDER = (0, 2, 1, 3)
Y_ORDER = (1, 3, 0, 2)
QUARTERS = 4
CHAIN_SHARE = 2
DUAL = (0, 1)
CHAIN = (2, 3)
scope = jax.named_scope


def flip(a, k):
    result = 0
    for bit in (1, 2, 4):
        own, other = (a // bit) % 2, (k // bit) % 2
        result = result + bit * (own + other - 2 * own * other)
    return result


def kernel(
    tok_in, gain_in, gate_in, up_in, down_in,
    wbuf, dbuf, layer_out,
    gain, w32, d32, dcast, xbuf, tbuf, acc, hidden, scale, keep, psend, precv, zsend, zrecv,
    load_g, load_t, load_w, load_d, tok_s, tok_r, w_s, w_r, dz_s, o_s, o_r, zr_s, d_s, d_r, p_s, p_r, z_s, z_r,
):
    f, t = lax.axis_index("fs"), lax.axis_index("tp")
    n_tp, n_fs = tbuf.shape[0], wbuf.shape[1]
    z, core = t // 2, t % 2
    fx, fy, fd = flip(f, 1), flip(f, 2), flip(f, 3)
    mate = flip(t, 1)
    base = t - core
    rows = wbuf.shape[2]
    part = rows // CHUNKS
    w_ins = (gate_in, up_in)
    tall, width = dbuf.shape[1], dbuf.shape[2]
    short = tall * CHAIN_SHARE // 16
    long = tall // 2 - short
    per = n_tp // n_fs
    n_tok = tbuf.shape[1]
    piece_rows = n_tok // n_tp
    n_z = n_tp // 2
    q = flip(f, z)
    side = jnp.logical_or(q == 1, q == 2)
    toward = fx + (fy - fx) * (q // 2)
    away = fy + (fx - fy) * (q // 2)

    def remote(src, dst, ss, rs, to_f, to_t):
        return pltpu.make_async_remote_copy(
            src_ref=src, dst_ref=dst, send_sem=ss, recv_sem=rs, device_id=(to_f, to_t), device_id_type=MESH
        )

    def load(w, i):
        return pltpu.make_async_copy(w_ins[w].at[pl.ds(i * part, part)], w32.at[w, pl.ds(i * part, part)], load_w.at[w, i])

    barrier = pltpu.get_barrier_semaphore()
    peers = [(fx, t), (fy, t)] + [(f, flip(t, k)) for k in range(1, n_tp)]
    for peer in peers:
        pl.semaphore_signal(barrier, inc=1, device_id=peer, device_id_type=MESH)

    load_gain = pltpu.make_async_copy(gain_in, gain, load_g)
    load_tok = pltpu.make_async_copy(tok_in, tbuf.at[t], load_t)
    load_down = [
        pltpu.make_async_copy(down_in.at[pl.ds(c * tall, tall)], d32.at[pl.ds(c * tall, tall)], load_d.at[c])
        for c in range(per)
    ]
    load_gain.start()
    for i in (0, 1):
        for w in range(2):
            load(w, i).start()
    load_tok.start()
    for copy in load_down:
        copy.start()
    for i in (2, 3):
        for w in range(2):
            load(w, i).start()

    def cast(w, i):
        block = pl.ds(i * part, part)
        load(w, i).wait()
        lanes = 128
        tall_gain = jnp.broadcast_to(gain[:, block], (lanes, part)).T
        for j in range(wbuf.shape[3] // lanes):
            columns = pl.ds(j * lanes, lanes)
            wbuf[w, f, block, columns] = (tall_gain * w32[w, block, columns]).astype(BF16)

    def tok_copy(piece, dz, to):
        return remote(tbuf.at[piece], tbuf.at[piece], tok_s, tok_r.at[dz], f, to)

    def w_copy(src, i, to):
        ref = wbuf.at[:, src, pl.ds(i * part, part)]
        return remote(ref, ref, w_s, w_r.at[src, i], to, t)

    def send_x(step):
        w_copy(f, X_ORDER[step], fx).start()

    def send_y(step):
        w_copy(f, Y_ORDER[step], fy).start()

    def send_own(step):
        send_x(step)
        send_y(step)

    def rows_of(h):
        return pl.ds(h * long, long) if h in DUAL else pl.ds(2 * long + (h - 2) * short, short)

    def dz_copy(c, h):
        return remote(dcast.at[c, rows_of(h)], dbuf.at[t, rows_of(h)], dz_s, d_r.at[t, h], f, f * per + c)

    def o_copy(slot, h, to):
        return remote(dcast.at[:, rows_of(h)], xbuf.at[slot, :, rows_of(h)], o_s, o_r.at[slot, h], to, t)

    def transit(h, to):
        ref = xbuf.at[2, :, rows_of(h)]
        return remote(ref, ref, o_s, o_r.at[2, h], to, t)

    def over_z(slot, c, h, column):
        return remote(xbuf.at[slot, c, rows_of(h)], dbuf.at[t, rows_of(h)], zr_s, d_r.at[t, h], f, column * per + c)

    def d_copy(piece, h, to):
        ref = dbuf.at[piece, rows_of(h)]
        return remote(ref, ref, d_s, d_r.at[piece, h], to, t)

    def sent(ref, sem):
        remote(ref, ref, sem, sem, fx, t).wait_send()

    chain_stops = (q == 2, q == 1)
    chain_to = (fx + (fy - fx) * (q % 2) * (1 - q // 2), fy + (fx - fy) * (1 - q % 2) * (q // 2))

    def chain(k, hs):
        piece = flip(base, k)
        for h in hs:
            @pl.when(jnp.logical_not(chain_stops[h % 2]))
            def _():
                if isinstance(k, int) and k < per:
                    @pl.when(jnp.logical_or(q != 0, core != k))
                    def _():
                        d_copy(piece, h, chain_to[h % 2]).wait_recv()
                else:
                    d_copy(piece, h, chain_to[h % 2]).wait_recv()
                d_copy(piece, h, chain_to[h % 2]).start()

    inner = jnp.logical_or(z == 1, z == 2)

    def chain_next(n):
        r = n // 2
        chain(2 * jnp.where(inner, 1 + r, 3 - r) + n % 2, CHAIN)

    def own_chain():
        for k in range(per):
            chain(k, range(QUARTERS))

    def hand(k, h, to):
        piece = flip(base, k)
        d_copy(piece, h, to).wait_recv()
        d_copy(piece, h, to).start()

    load_gain.wait()
    cast(0, X_ORDER[0])
    cast(1, X_ORDER[0])
    with scope("barrier"):
        pl.semaphore_wait(barrier, len(peers))
    cast(0, Y_ORDER[0])
    send_x(0)
    cast(1, Y_ORDER[0])
    send_y(0)
    load_tok.wait()
    for dz, k in enumerate((1, 2, 4, 6)):
        tok_copy(t, dz, flip(t, k)).start()

    for c in range(per):
        load_down[c].wait()
        for h in range(QUARTERS):
            block = rows_of(h)
            dcast[c, block] = d32[pl.ds(c * tall + block.start, block.size)].astype(BF16)

        @pl.when(t == f * per + c)
        def _():
            dbuf[t] = dcast[c]

    cast(0, X_ORDER[1])
    cast(0, Y_ORDER[1])

    @pl.when(side)
    def _():
        for h in DUAL:
            o_copy(q - 1, h, toward).start()

    @pl.when(q == 3)
    def _():
        o_copy(2, 0, fx).start()
        o_copy(2, 1, fy).start()

    for h in CHAIN + DUAL:
        for c in range(per):
            @pl.when(t != f * per + c)
            def _():
                dz_copy(c, h).start()

    cast(1, X_ORDER[1])
    cast(1, Y_ORDER[1])

    @pl.when(q == 0)
    def _():
        own_chain()

    send_own(1)

    def arrive(step):
        w_copy(fx, X_ORDER[step], fy).wait_recv()
        w_copy(fy, Y_ORDER[step], fx).wait_recv()

    def forward(step):
        w_copy(fx, X_ORDER[step], fy).start()
        w_copy(fy, Y_ORDER[step], fx).start()

    with scope("arrive0"):
        arrive(0)
    with scope("transit"):
        for way in range(2):
            @pl.when(q == 1 + way)
            def _():
                transit(1 - way, toward).wait_recv()
                transit(1 - way, toward).start()
                for c in range(per):
                    over_z(2, c, 1 - way, away).start()

    send_own(2)

    with scope("own_chain"):
        @pl.when(side)
        def _():
            own_chain()

    send_own(3)

    with scope("over_z"):
        @pl.when(q == 0)
        def _():
            for h in DUAL:
                for slot, column in enumerate((fx, fy)):
                    o_copy(slot, h, fx).wait_recv()
                    for c in range(per):
                        over_z(slot, c, h, column).start()

    with scope("arrive1"):
        forward(0)
        arrive(1)

    with scope("over_z2"):
        @pl.when(q == 0)
        def _():
            for h in DUAL:
                o_copy(2, h, fx).wait_recv()
                for c in range(per):
                    over_z(2, c, h, fd).start()

    with scope("chain0"):
        @pl.when(q == 0)
        def _():
            chain_next(0)
            chain_next(1)

    forward(1)

    tile = 512

    def accumulate(src, first, parts=range(per)):
        def one(n, _):
            w, column = n // (wbuf.shape[3] // tile), pl.multiple_of(n % (wbuf.shape[3] // tile) * tile, tile)
            total = 0.0 if first else acc[w, :, pl.ds(column, tile)]
            for p in parts:
                total = total + jnp.dot(
                    tbuf[src * per + p],
                    wbuf[w, src, pl.ds(p * width, width), pl.ds(column, tile)],
                    preferred_element_type=F32,
                )
            acc[w, :, pl.ds(column, tile)] = total
            return 0

        lax.fori_loop(0, 2 * (wbuf.shape[3] // tile), one, 0)

    with scope("tokens"):
        for dz in range(1, n_z):
            piece = flip(t, 2 * dz)
            tok_copy(piece, dz, mate).wait_recv()
            tok_copy(piece, 0, mate).start()
        remote(tbuf.at[pl.ds(0, n_z)], tbuf.at[pl.ds(0, n_z)], tok_s, tok_r.at[0], f, mate).wait_recv()

    with scope("own_chain3"):
        @pl.when(q == 3)
        def _():
            own_chain()

    def norm(i, _):
        block = pl.ds(i * piece_rows, piece_rows)
        squares = 0.0
        for p in range(n_tp):
            wide = tbuf[p, block].astype(F32)
            squares = squares + wide * wide
        scale[block] = lax.rsqrt(jnp.sum(squares, axis=1, keepdims=True) / (n_tp * width) + epsilon)
        return 0

    with scope("norm"):
        lax.fori_loop(0, n_tp, norm, 0)
    with scope("own_dot"):
        accumulate(f, True)
    with scope("arrive23"):
        for step in range(CHUNKS // 2, CHUNKS):
            arrive(step)
    with scope("fx_dot"):
        accumulate(fx, False)
    with scope("fy_dot"):
        accumulate(fy, False)

    with scope("early"):
        @pl.when(q == 0)
        def _():
            for n in range(2, 6):
                chain_next(n)
            for k, to in ((4, fx), (5, fx), (2, fy), (3, fy)):
                for h in DUAL:
                    hand(k, h, to)

        for place, k, to in ((1, 2, fy), (2, 4, fx)):
            @pl.when(q == place)
            def _():
                chain_next(0)
                chain_next(1)
                for h in DUAL:
                    hand(k, h, to)
                    d_copy(flip(base, k + 1), h, to).wait_recv()

        @pl.when(q == 3)
        def _():
            hand(6, 0, fx)
            hand(6, 1, fy)

    for p in range(per):
        with scope("fd_wait"):
            for i in (2 * p, 2 * p + 1):
                w_copy(fd, i, fx).wait_recv()
        with scope("fd_dot"):
            accumulate(fd, False, (p,))

    def make_hidden(n, _):
        columns = pl.ds(pl.multiple_of(n * tile, tile), tile)
        s = scale[...]
        g = acc[0, :, columns] * s
        hidden[:, columns] = (g / (1.0 + jnp.exp(-g)) * (acc[1, :, columns] * s)).astype(BF16)
        return 0

    with scope("hidden"):
        lax.fori_loop(0, hidden.shape[1] // tile, make_hidden, 0)

    def p_copy(k):
        return remote(psend.at[k], precv.at[k], p_s, p_r.at[k], f, mate)

    def z_copy(k, dz, piece):
        to = flip(t, 2 * dz)
        return remote(zsend.at[k, to // 2], zrecv.at[z, piece], z_s, z_r.at[piece], f, to)

    def finish(k):
        p_copy(k).wait_recv()
        for b in range(n_z):
            zsend[k, b] = (keep[k, b] + precv[k, b].astype(F32)).astype(BF16)
        piece = flip(base, k)
        zrecv[z, piece] = zsend[k, z]
        for dz in range(1, n_z):
            z_copy(k, dz, piece).start()

    def product(k):
        piece = flip(base, k)
        out = jnp.dot(hidden[...], dbuf[piece], preferred_element_type=F32)
        out = out.reshape(n_z, 2, piece_rows, width)

        @pl.when(core == 0)
        def _():
            keep[k] = out[:, 0]
            psend[k] = out[:, 1].astype(BF16)

        @pl.when(core == 1)
        def _():
            keep[k] = out[:, 1]
            psend[k] = out[:, 0].astype(BF16)

        p_copy(k).start()

    def take(k):
        piece = flip(base, k)
        r = k // 2
        passed = jnp.logical_or(
            jnp.logical_or(jnp.logical_and(r == 1, q < 2), jnp.logical_and(r == 2, q % 2 == 0)),
            jnp.logical_and(r == 3, q == 3),
        )

        @pl.when(jnp.logical_and(r > 0, jnp.logical_not(passed)))
        def _():
            for h in DUAL:
                d_copy(piece, h, fx).wait_recv()

        for side_h in range(2):
            @pl.when(chain_stops[side_h])
            def _():
                d_copy(piece, CHAIN[side_h], fx).wait_recv()

                @pl.when(r == 0)
                def _():
                    d_copy(piece, DUAL[side_h], fx).wait_recv()

    def turn(i):
        k = i
        for here, order in (
            (jnp.logical_and(inner, q == 1), (0, 1, 2, 3, 4, 6, 5, 7)),
            (jnp.logical_and(inner, q == 2), (0, 1, 2, 4, 5, 6, 3, 7)),
            (jnp.logical_and(inner, q == 3), (0, 1, 2, 4, 6, 7, 3, 5)),
            (jnp.logical_and(jnp.logical_not(inner), q % 2 == 0), (0, 1, 6, 7, 4, 5, 2, 3)),
            (jnp.logical_and(jnp.logical_not(inner), q % 2 == 1), (0, 1, 6, 7, 4, 2, 5, 3)),
        ):
            mine = 0
            for n, v in enumerate(order):
                mine = mine + v * jnp.where(i == n, 1, 0)
            k = jnp.where(here, mine, k)
        return k

    def pass_on(i):
        @pl.when(jnp.logical_and(side, i == 2))
        def _():
            for n in range(2, 6):
                chain_next(n)

        for place, k, to in ((1, 3, fy), (2, 5, fx)):
            @pl.when(jnp.logical_and(q == place, i == 2))
            def _():
                for h in DUAL:
                    d_copy(flip(base, k), h, to).start()

        @pl.when(jnp.logical_and(q == 3, i == 2))
        def _():
            chain_next(0)
            chain_next(1)
            hand(7, 0, fx)
            hand(7, 1, fy)

        @pl.when(jnp.logical_and(q == 3, jnp.logical_and(i >= 3, i <= 4)))
        def _():
            chain_next(2 * i - 4)
            chain_next(2 * i - 3)

    def step(i, _):
        with scope("pass_on"):
            pass_on(i)

        last = i - 1 - jnp.where(jnp.logical_or(q == 0, i >= n_tp), 1, 0)
        now = jnp.logical_or(q == 0, i != n_tp - 1)

        @pl.when(jnp.logical_and(now, jnp.logical_and(last >= 0, last < n_tp)))
        def _():
            with scope("finish"):
                finish(turn(last))

        @pl.when(i < n_tp)
        def _():
            k = turn(i)
            with scope("take"):
                take(k)
            with scope("product"):
                product(k)

        return 0

    lax.fori_loop(0, n_tp + 2, step, 0)

    with scope("sent"):
        sent(tbuf.at[pl.ds(0, n_tp - 1)], tok_s)
        sent(wbuf.at[:, pl.ds(0, n_fs - 1)], w_s)
        sent(psend, p_s)

        @pl.when(q == 0)
        def _():
            sent(dcast.at[0], dz_s)
            sent(xbuf, zr_s)
            sent(dbuf.at[:, pl.ds(0, 3 * tall // 4 + short // 2)], d_s)

        @pl.when(side)
        def _():
            sent(xbuf.at[:, :, rows_of(0)], o_s)
            sent(xbuf.at[0, 0], zr_s)
            sent(dbuf.at[:, pl.ds(0, 3 * tall // 8 + short // 4)], d_s)

        @pl.when(q == 3)
        def _():
            sent(xbuf.at[0], o_s)
            sent(dbuf.at[:, pl.ds(0, tall // 2 + short)], d_s)

        @pl.when(q != 0)
        def _():
            sent(dcast, dz_s)

    for piece in range(n_tp):
        with scope("z_wait"):
            others = zrecv.at[pl.ds(0, n_z - 1), piece]
            remote(others, others, z_s, z_r.at[piece], f, mate).wait_recv()
        total = zrecv[0, piece].astype(F32)
        for b in range(1, n_z):
            total = total + zrecv[b, piece].astype(F32)
        layer_out[:, pl.ds(piece * width, width)] = total.astype(BF16)
    sent(zsend.at[:, pl.ds(0, n_z - 1)], z_s)


def write_out(weights, down, layer, gate_out, up_out, down_out, layer_out, w_s, d_s, l_s):
    _, n_fs, rows, _ = weights.shape
    n_tp, _, width = down.shape
    copies = [pltpu.make_async_copy(layer, layer_out, l_s)]
    for w, out in enumerate((gate_out, up_out)):
        for src in range(n_fs):
            copies.append(pltpu.make_async_copy(weights.at[w, src], out.at[pl.ds(src * rows, rows)], w_s.at[w, src]))
    for j in range(n_tp):
        copies.append(pltpu.make_async_copy(down.at[j], down_out.at[:, pl.ds(j * width, width)], d_s.at[j]))
    for copy in copies:
        copy.start()
    for copy in copies:
        copy.wait()


def body(tokens, norm_gain, gate_train, up_train, down_train, *, n_fs, n_tp):
    n_tok, width = tokens.shape
    rows, cols = gate_train.shape
    tall = down_train.shape[0] * n_fs // n_tp
    piece_rows = n_tok // n_tp
    n_z = n_tp // 2
    hbm = pl.BlockSpec(memory_space=pltpu.HBM)
    vmem = pl.BlockSpec(memory_space=pltpu.VMEM)
    dma = pltpu.SemaphoreType.DMA
    weights, down, layer = pl.pallas_call(
        kernel,
        out_shape=(
            pltpu.VMEM((2, n_fs, rows, cols), BF16),
            pltpu.VMEM((n_tp, tall, width), BF16),
            pltpu.VMEM((piece_rows, width * n_tp), BF16),
        ),
        in_specs=[hbm] * 5,
        out_specs=(vmem, vmem, vmem),
        scratch_shapes=[
            pltpu.VMEM((1, rows), F32),
            pltpu.VMEM((2, rows, cols), F32),
            pltpu.VMEM(down_train.shape, F32),
            pltpu.VMEM((n_tp // n_fs, tall, width), BF16),
            pltpu.VMEM((3, n_tp // n_fs, tall - tall * CHAIN_SHARE // 8, width), BF16),
            pltpu.VMEM((n_tp, n_tok, width), BF16),
            pltpu.VMEM((2, n_tok, cols), F32),
            pltpu.VMEM((n_tok, cols), BF16),
            pltpu.VMEM((n_tok, 1), F32),
            pltpu.VMEM((n_tp, n_z, piece_rows, width), F32),
            pltpu.VMEM((n_tp, n_z, piece_rows, width), BF16),
            pltpu.VMEM((n_tp, n_z, piece_rows, width), BF16),
            pltpu.VMEM((n_tp, n_z, piece_rows, width), BF16),
            pltpu.VMEM((n_z, n_tp, piece_rows, width), BF16),
            dma,
            dma,
            dma((2, CHUNKS)),
            dma((n_tp // n_fs,)),
            dma,
            dma((n_z,)),
            dma,
            dma((n_fs, CHUNKS)),
            dma,
            dma,
            dma((3, len(DUAL))),
            dma,
            dma,
            dma((n_tp, QUARTERS)),
            dma,
            dma((n_tp,)),
            dma,
            dma((n_tp,)),
        ],
        compiler_params=pltpu.CompilerParams(
            collective_id=0, has_side_effects=True, vmem_limit_bytes=51 * 1024 * 1024
        ),
    )(tokens, norm_gain[None, :], gate_train, up_train, down_train)
    return pl.pallas_call(
        write_out,
        out_shape=(
            jax.ShapeDtypeStruct((rows * n_fs, cols), BF16),
            jax.ShapeDtypeStruct((rows * n_fs, cols), BF16),
            jax.ShapeDtypeStruct((tall, width * n_tp), BF16),
            jax.ShapeDtypeStruct((piece_rows, width * n_tp), BF16),
        ),
        in_specs=[vmem] * 3,
        out_specs=(pl.BlockSpec(memory_space=pl.ANY),) * 4,
        scratch_shapes=[dma((2, n_fs)), dma((n_tp,)), dma],
        compiler_params=pltpu.CompilerParams(vmem_limit_bytes=4 * 1024 * 1024),
    )(weights, down, layer)


def plain(tokens, norm_gain, gate_train, up_train, down_train):
    gate_local = (norm_gain[:, None] * gate_train).astype(BF16)
    up_local = (norm_gain[:, None] * up_train).astype(BF16)
    down_local = down_train.astype(BF16)
    features = lax.all_gather(tokens, "tp", axis=1, tiled=True)
    wide = features.astype(F32)
    squares = jnp.sum(wide * wide, axis=1)
    gate_whole = lax.all_gather(gate_local, "fs", axis=0, tiled=True)
    up_whole = lax.all_gather(up_local, "fs", axis=0, tiled=True)
    gate_sum = jnp.dot(features, gate_whole, preferred_element_type=F32)
    up_sum = jnp.dot(features, up_whole, preferred_element_type=F32)
    down_rows = lax.all_gather(down_local, "fs", axis=0, tiled=True)
    down_whole = lax.all_to_all(down_rows, "tp", split_axis=0, concat_axis=1, tiled=True)
    scale = lax.rsqrt(squares / features.shape[1] + epsilon)[:, None]
    hidden = (jax.nn.silu(gate_sum * scale) * (up_sum * scale)).astype(BF16)
    mixed = lax.psum_scatter(
        jnp.dot(hidden, down_whole, preferred_element_type=F32).astype(BF16), "tp", scatter_dimension=0, tiled=True
    )
    return (gate_whole, up_whole, down_whole, mixed)


def solution(mesh):
    n_fs, n_tp = mesh.shape["fs"], mesh.shape["tp"]
    fast = n_fs == 4 and n_tp == 8
    return jax.shard_map(
        functools.partial(body, n_fs=n_fs, n_tp=n_tp) if fast else plain,
        mesh=mesh,
        in_specs=(P("fs", "tp"), P("fs"), P("fs", "tp"), P("fs", "tp"), P("fs", "tp")),
        out_specs=(P(None, "tp"), P(None, "tp"), P("tp", None), P(("fs", "tp"), None)),
        check_vma=False,
    )
```

```python
import functools

import jax
import jax.numpy as jnp
from jax import lax
from jax.experimental import pallas as pl
from jax.experimental.pallas import tpu as pltpu
from jax.sharding import PartitionSpec as P

MESH = pl.DeviceIdType.MESH
BF16 = jnp.bfloat16
F32 = jnp.float32
epsilon = 1e-06
CHUNKS = 4
X_ORDER = (0, 2, 1, 3)
Y_ORDER = (1, 3, 0, 2)
QUARTERS = 4
CHAIN_SHARE = 5
DUAL = (0, 1)
CHAIN = (2, 3)
scope = jax.named_scope


def flip(a, k):
    result = 0
    for bit in (1, 2, 4):
        own, other = (a // bit) % 2, (k // bit) % 2
        result = result + bit * (own + other - 2 * own * other)
    return result


def kernel(
    tok_in, gain_in, gate_in, up_in, down_in,
    wbuf, dbuf, layer_out,
    gain, w32, d32, dcast, xbuf, tbuf, acc, hidden, scale, keep, psend, precv, zsend, zrecv,
    load_g, load_t, load_w, load_d, tok_s, tok_r, w_s, w_r, dz_s, o_s, o_r, zr_s, d_s, d_r, p_s, p_r, z_s, z_r,
):
    f, t = lax.axis_index("fs"), lax.axis_index("tp")
    n_tp, n_fs = tbuf.shape[0], wbuf.shape[1]
    z, core = t // 2, t % 2
    fx, fy, fd = flip(f, 1), flip(f, 2), flip(f, 3)
    mate = flip(t, 1)
    base = t - core
    rows = wbuf.shape[2]
    part = rows // CHUNKS
    w_ins = (gate_in, up_in)
    tall, width = dbuf.shape[1], dbuf.shape[2]
    short = tall * CHAIN_SHARE // 32
    long = tall // 2 - short
    per = n_tp // n_fs
    n_tok = tbuf.shape[1]
    piece_rows = n_tok // n_tp
    n_z = n_tp // 2
    q = flip(f, z)
    side = jnp.logical_or(q == 1, q == 2)
    toward = fx + (fy - fx) * (q // 2)
    away = fy + (fx - fy) * (q // 2)

    def remote(src, dst, ss, rs, to_f, to_t):
        return pltpu.make_async_remote_copy(
            src_ref=src, dst_ref=dst, send_sem=ss, recv_sem=rs, device_id=(to_f, to_t), device_id_type=MESH
        )

    def load(w, i):
        return pltpu.make_async_copy(w_ins[w].at[pl.ds(i * part, part)], w32.at[w, pl.ds(i * part, part)], load_w.at[w, i])

    barrier = pltpu.get_barrier_semaphore()
    peers = [(fx, t), (fy, t)] + [(f, flip(t, k)) for k in range(1, n_tp)]
    for peer in peers:
        pl.semaphore_signal(barrier, inc=1, device_id=peer, device_id_type=MESH)

    load_gain = pltpu.make_async_copy(gain_in, gain, load_g)
    load_tok = pltpu.make_async_copy(tok_in, tbuf.at[t], load_t)
    load_down = [
        pltpu.make_async_copy(down_in.at[pl.ds(c * tall, tall)], d32.at[pl.ds(c * tall, tall)], load_d.at[c])
        for c in range(per)
    ]
    load_gain.start()
    for i in (0, 1):
        for w in range(2):
            load(w, i).start()
    load_tok.start()
    for copy in load_down:
        copy.start()
    for i in (2, 3):
        for w in range(2):
            load(w, i).start()

    def cast(w, i):
        block = pl.ds(i * part, part)
        load(w, i).wait()
        lanes = 128
        tall_gain = jnp.broadcast_to(gain[:, block], (lanes, part)).T
        for j in range(wbuf.shape[3] // lanes):
            columns = pl.ds(j * lanes, lanes)
            wbuf[w, f, block, columns] = (tall_gain * w32[w, block, columns]).astype(BF16)

    def tok_copy(piece, dz, to):
        return remote(tbuf.at[piece], tbuf.at[piece], tok_s, tok_r.at[dz], f, to)

    def w_copy(src, i, to):
        ref = wbuf.at[:, src, pl.ds(i * part, part)]
        return remote(ref, ref, w_s, w_r.at[src, i], to, t)

    def send_x(step):
        w_copy(f, X_ORDER[step], fx).start()

    def send_y(step):
        w_copy(f, Y_ORDER[step], fy).start()

    def send_own(step):
        send_x(step)
        send_y(step)

    def rows_of(h):
        return pl.ds(h * long, long) if h in DUAL else pl.ds(2 * long + (h - 2) * short, short)

    def dz_copy(c, h):
        return remote(dcast.at[c, rows_of(h)], dbuf.at[t, rows_of(h)], dz_s, d_r.at[t, h], f, f * per + c)

    def o_copy(slot, h, to):
        return remote(dcast.at[:, rows_of(h)], xbuf.at[slot, :, rows_of(h)], o_s, o_r.at[slot, h], to, t)

    def transit(h, to):
        ref = xbuf.at[2, :, rows_of(h)]
        return remote(ref, ref, o_s, o_r.at[2, h], to, t)

    def over_z(slot, c, h, column):
        return remote(xbuf.at[slot, c, rows_of(h)], dbuf.at[t, rows_of(h)], zr_s, d_r.at[t, h], f, column * per + c)

    def d_copy(piece, h, to):
        ref = dbuf.at[piece, rows_of(h)]
        return remote(ref, ref, d_s, d_r.at[piece, h], to, t)

    def sent(ref, sem):
        remote(ref, ref, sem, sem, fx, t).wait_send()

    chain_stops = (q == 2, q == 1)
    chain_to = (fx + (fy - fx) * (q % 2) * (1 - q // 2), fy + (fx - fy) * (1 - q % 2) * (q // 2))

    def chain(k, hs):
        piece = flip(base, k)
        for h in hs:
            @pl.when(jnp.logical_not(chain_stops[h % 2]))
            def _():
                if isinstance(k, int) and k < per:
                    @pl.when(jnp.logical_or(q != 0, core != k))
                    def _():
                        d_copy(piece, h, chain_to[h % 2]).wait_recv()
                else:
                    d_copy(piece, h, chain_to[h % 2]).wait_recv()
                d_copy(piece, h, chain_to[h % 2]).start()

    inner = jnp.logical_or(z == 1, z == 2)

    def chain_next(n):
        r = n // 2
        chain(2 * jnp.where(inner, 1 + r, 3 - r) + n % 2, CHAIN)

    def own_chain():
        for k in range(per):
            chain(k, range(QUARTERS))

    def hand(k, h, to):
        piece = flip(base, k)
        d_copy(piece, h, to).wait_recv()
        d_copy(piece, h, to).start()

    load_gain.wait()
    cast(0, X_ORDER[0])
    cast(1, X_ORDER[0])
    with scope("barrier"):
        pl.semaphore_wait(barrier, len(peers))
    cast(0, Y_ORDER[0])
    send_x(0)
    cast(1, Y_ORDER[0])
    send_y(0)
    load_tok.wait()
    for dz, k in enumerate((1, 2, 4, 6)):
        tok_copy(t, dz, flip(t, k)).start()

    for c in range(per):
        load_down[c].wait()
        for h in range(QUARTERS):
            block = rows_of(h)
            dcast[c, block] = d32[pl.ds(c * tall + block.start, block.size)].astype(BF16)

        @pl.when(t == f * per + c)
        def _():
            dbuf[t] = dcast[c]

    cast(0, X_ORDER[1])
    cast(0, Y_ORDER[1])

    @pl.when(side)
    def _():
        for h in DUAL:
            o_copy(q - 1, h, toward).start()

    @pl.when(q == 3)
    def _():
        o_copy(2, 0, fx).start()
        o_copy(2, 1, fy).start()

    for h in CHAIN + DUAL:
        for c in range(per):
            @pl.when(t != f * per + c)
            def _():
                dz_copy(c, h).start()

    cast(1, X_ORDER[1])
    cast(1, Y_ORDER[1])

    @pl.when(q == 0)
    def _():
        own_chain()

    send_own(1)

    def arrive(step):
        w_copy(fx, X_ORDER[step], fy).wait_recv()
        w_copy(fy, Y_ORDER[step], fx).wait_recv()

    def forward(step):
        w_copy(fx, X_ORDER[step], fy).start()
        w_copy(fy, Y_ORDER[step], fx).start()

    with scope("arrive0"):
        arrive(0)
    with scope("transit"):
        for way in range(2):
            @pl.when(q == 1 + way)
            def _():
                transit(1 - way, toward).wait_recv()
                transit(1 - way, toward).start()
                for c in range(per):
                    over_z(2, c, 1 - way, away).start()

    send_own(2)

    with scope("own_chain"):
        @pl.when(side)
        def _():
            own_chain()

    send_own(3)

    with scope("over_z"):
        @pl.when(q == 0)
        def _():
            for h in DUAL:
                for slot, column in enumerate((fx, fy)):
                    o_copy(slot, h, fx).wait_recv()
                    for c in range(per):
                        over_z(slot, c, h, column).start()

    with scope("arrive1"):
        forward(0)
        arrive(1)

    with scope("over_z2"):
        @pl.when(q == 0)
        def _():
            for h in DUAL:
                o_copy(2, h, fx).wait_recv()
                for c in range(per):
                    over_z(2, c, h, fd).start()

    with scope("chain0"):
        @pl.when(q == 0)
        def _():
            chain_next(0)
            chain_next(1)

    forward(1)

    tile = 512

    def accumulate(src, first, parts=range(per)):
        def one(n, _):
            w, column = n // (wbuf.shape[3] // tile), pl.multiple_of(n % (wbuf.shape[3] // tile) * tile, tile)
            total = 0.0 if first else acc[w, :, pl.ds(column, tile)]
            for p in parts:
                total = total + jnp.dot(
                    tbuf[src * per + p],
                    wbuf[w, src, pl.ds(p * width, width), pl.ds(column, tile)],
                    preferred_element_type=F32,
                )
            acc[w, :, pl.ds(column, tile)] = total
            return 0

        lax.fori_loop(0, 2 * (wbuf.shape[3] // tile), one, 0)

    with scope("tokens"):
        for dz in range(1, n_z):
            piece = flip(t, 2 * dz)
            tok_copy(piece, dz, mate).wait_recv()
            tok_copy(piece, 0, mate).start()
        remote(tbuf.at[pl.ds(0, n_z)], tbuf.at[pl.ds(0, n_z)], tok_s, tok_r.at[0], f, mate).wait_recv()

    with scope("own_chain3"):
        @pl.when(q == 3)
        def _():
            own_chain()

    def norm(i, _):
        block = pl.ds(i * piece_rows, piece_rows)
        squares = 0.0
        for p in range(n_tp):
            wide = tbuf[p, block].astype(F32)
            squares = squares + wide * wide
        scale[block] = lax.rsqrt(jnp.sum(squares, axis=1, keepdims=True) / (n_tp * width) + epsilon)
        return 0

    with scope("norm"):
        lax.fori_loop(0, n_tp, norm, 0)
    with scope("own_dot"):
        accumulate(f, True)
    with scope("arrive23"):
        for step in range(CHUNKS // 2, CHUNKS):
            arrive(step)
    with scope("fx_dot"):
        accumulate(fx, False)
    with scope("fy_dot"):
        accumulate(fy, False)

    with scope("early"):
        @pl.when(q == 0)
        def _():
            for n in range(2, 6):
                chain_next(n)
            for k, to in ((4, fx), (5, fx), (2, fy), (3, fy)):
                for h in DUAL:
                    hand(k, h, to)

        for place, k, to in ((1, 2, fy), (2, 4, fx)):
            @pl.when(q == place)
            def _():
                chain_next(0)
                chain_next(1)
                for h in DUAL:
                    hand(k, h, to)
                    d_copy(flip(base, k + 1), h, to).wait_recv()

        @pl.when(q == 3)
        def _():
            hand(6, 0, fx)
            hand(6, 1, fy)

    for p in range(per):
        with scope("fd_wait"):
            for i in (2 * p, 2 * p + 1):
                w_copy(fd, i, fx).wait_recv()
        with scope("fd_dot"):
            accumulate(fd, False, (p,))

    def make_hidden(n, _):
        columns = pl.ds(pl.multiple_of(n * tile, tile), tile)
        s = scale[...]
        g = acc[0, :, columns] * s
        hidden[:, columns] = (g / (1.0 + jnp.exp(-g)) * (acc[1, :, columns] * s)).astype(BF16)
        return 0

    with scope("hidden"):
        lax.fori_loop(0, hidden.shape[1] // tile, make_hidden, 0)

    def p_copy(k):
        return remote(psend.at[k], precv.at[k], p_s, p_r.at[k], f, mate)

    def z_copy(k, dz, piece):
        to = flip(t, 2 * dz)
        return remote(zsend.at[k, to // 2], zrecv.at[z, piece], z_s, z_r.at[piece], f, to)

    def finish(k):
        p_copy(k).wait_recv()
        for b in range(n_z):
            zsend[k, b] = (keep[k, b] + precv[k, b].astype(F32)).astype(BF16)
        piece = flip(base, k)
        zrecv[z, piece] = zsend[k, z]
        far = jnp.where(inner, 2, 3)
        for dz in (far, 5 - far, 1):
            z_copy(k, dz, piece).start()

    def product(k):
        piece = flip(base, k)
        out = jnp.dot(hidden[...], dbuf[piece], preferred_element_type=F32)
        out = out.reshape(n_z, 2, piece_rows, width)

        @pl.when(core == 0)
        def _():
            keep[k] = out[:, 0]
            psend[k] = out[:, 1].astype(BF16)

        @pl.when(core == 1)
        def _():
            keep[k] = out[:, 1]
            psend[k] = out[:, 0].astype(BF16)

        p_copy(k).start()

    def take(k):
        piece = flip(base, k)
        r = k // 2
        passed = jnp.logical_or(
            jnp.logical_or(jnp.logical_and(r == 1, q < 2), jnp.logical_and(r == 2, q % 2 == 0)),
            jnp.logical_and(r == 3, q == 3),
        )

        @pl.when(jnp.logical_and(r > 0, jnp.logical_not(passed)))
        def _():
            for h in DUAL:
                d_copy(piece, h, fx).wait_recv()

        for side_h in range(2):
            @pl.when(chain_stops[side_h])
            def _():
                d_copy(piece, CHAIN[side_h], fx).wait_recv()

                @pl.when(r == 0)
                def _():
                    d_copy(piece, DUAL[side_h], fx).wait_recv()

    def turn(i):
        k = i
        for here, order in (
            (jnp.logical_and(inner, q == 1), (0, 1, 2, 3, 4, 6, 5, 7)),
            (jnp.logical_and(inner, q == 2), (0, 1, 2, 4, 5, 6, 3, 7)),
            (jnp.logical_and(inner, q == 3), (0, 1, 2, 4, 6, 7, 3, 5)),
            (jnp.logical_and(jnp.logical_not(inner), q % 2 == 0), (0, 1, 6, 7, 4, 5, 2, 3)),
            (jnp.logical_and(jnp.logical_not(inner), q % 2 == 1), (0, 1, 6, 7, 4, 2, 5, 3)),
        ):
            mine = 0
            for n, v in enumerate(order):
                mine = mine + v * jnp.where(i == n, 1, 0)
            k = jnp.where(here, mine, k)
        return k

    def pass_on(i):
        @pl.when(jnp.logical_and(side, i == 2))
        def _():
            for n in range(2, 6):
                chain_next(n)

        for place, k, to in ((1, 3, fy), (2, 5, fx)):
            @pl.when(jnp.logical_and(q == place, i == 2))
            def _():
                for h in DUAL:
                    d_copy(flip(base, k), h, to).start()

        @pl.when(jnp.logical_and(q == 3, i == 2))
        def _():
            chain_next(0)
            chain_next(1)
            hand(7, 0, fx)
            hand(7, 1, fy)

        @pl.when(jnp.logical_and(q == 3, jnp.logical_and(i >= 3, i <= 4)))
        def _():
            chain_next(2 * i - 4)
            chain_next(2 * i - 3)

    def step(i, _):
        with scope("pass_on"):
            pass_on(i)

        last = i - 1 - jnp.where(jnp.logical_or(q == 0, i >= n_tp), 1, 0)
        now = jnp.logical_or(q == 0, i != n_tp - 1)

        @pl.when(jnp.logical_and(now, jnp.logical_and(last >= 0, last < n_tp)))
        def _():
            with scope("finish"):
                finish(turn(last))

        @pl.when(i < n_tp)
        def _():
            k = turn(i)
            with scope("take"):
                take(k)
            with scope("product"):
                product(k)

        return 0

    lax.fori_loop(0, n_tp + 2, step, 0)

    with scope("sent"):
        sent(tbuf.at[pl.ds(0, n_tp - 1)], tok_s)
        sent(wbuf.at[:, pl.ds(0, n_fs - 1)], w_s)
        sent(psend, p_s)

        @pl.when(q == 0)
        def _():
            sent(dcast.at[0], dz_s)
            sent(xbuf, zr_s)
            sent(dbuf.at[:, pl.ds(0, 3 * tall // 4 + short // 2)], d_s)

        @pl.when(side)
        def _():
            sent(xbuf.at[:, :, rows_of(0)], o_s)
            sent(xbuf.at[0, 0], zr_s)
            sent(dbuf.at[:, pl.ds(0, 3 * tall // 8 + short // 4)], d_s)

        @pl.when(q == 3)
        def _():
            sent(xbuf.at[0], o_s)
            sent(dbuf.at[:, pl.ds(0, tall // 2 + short)], d_s)

        @pl.when(q != 0)
        def _():
            sent(dcast, dz_s)

    for piece in range(n_tp):
        with scope("z_wait"):
            others = zrecv.at[pl.ds(0, n_z - 1), piece]
            remote(others, others, z_s, z_r.at[piece], f, mate).wait_recv()
        total = zrecv[0, piece].astype(F32)
        for b in range(1, n_z):
            total = total + zrecv[b, piece].astype(F32)
        layer_out[:, pl.ds(piece * width, width)] = total.astype(BF16)
    sent(zsend.at[:, pl.ds(0, n_z - 1)], z_s)


def write_out(weights, down, layer, gate_out, up_out, down_out, layer_out, w_s, d_s, l_s):
    _, n_fs, rows, _ = weights.shape
    n_tp, _, width = down.shape
    copies = [pltpu.make_async_copy(layer, layer_out, l_s)]
    for w, out in enumerate((gate_out, up_out)):
        for src in range(n_fs):
            copies.append(pltpu.make_async_copy(weights.at[w, src], out.at[pl.ds(src * rows, rows)], w_s.at[w, src]))
    for j in range(n_tp):
        copies.append(pltpu.make_async_copy(down.at[j], down_out.at[:, pl.ds(j * width, width)], d_s.at[j]))
    for copy in copies:
        copy.start()
    for copy in copies:
        copy.wait()


def body(tokens, norm_gain, gate_train, up_train, down_train, *, n_fs, n_tp):
    n_tok, width = tokens.shape
    rows, cols = gate_train.shape
    tall = down_train.shape[0] * n_fs // n_tp
    piece_rows = n_tok // n_tp
    n_z = n_tp // 2
    hbm = pl.BlockSpec(memory_space=pltpu.HBM)
    vmem = pl.BlockSpec(memory_space=pltpu.VMEM)
    dma = pltpu.SemaphoreType.DMA
    weights, down, layer = pl.pallas_call(
        kernel,
        out_shape=(
            pltpu.VMEM((2, n_fs, rows, cols), BF16),
            pltpu.VMEM((n_tp, tall, width), BF16),
            pltpu.VMEM((piece_rows, width * n_tp), BF16),
        ),
        in_specs=[hbm] * 5,
        out_specs=(vmem, vmem, vmem),
        scratch_shapes=[
            pltpu.VMEM((1, rows), F32),
            pltpu.VMEM((2, rows, cols), F32),
            pltpu.VMEM(down_train.shape, F32),
            pltpu.VMEM((n_tp // n_fs, tall, width), BF16),
            pltpu.VMEM((3, n_tp // n_fs, tall - tall * CHAIN_SHARE // 16, width), BF16),
            pltpu.VMEM((n_tp, n_tok, width), BF16),
            pltpu.VMEM((2, n_tok, cols), F32),
            pltpu.VMEM((n_tok, cols), BF16),
            pltpu.VMEM((n_tok, 1), F32),
            pltpu.VMEM((n_tp, n_z, piece_rows, width), F32),
            pltpu.VMEM((n_tp, n_z, piece_rows, width), BF16),
            pltpu.VMEM((n_tp, n_z, piece_rows, width), BF16),
            pltpu.VMEM((n_tp, n_z, piece_rows, width), BF16),
            pltpu.VMEM((n_z, n_tp, piece_rows, width), BF16),
            dma,
            dma,
            dma((2, CHUNKS)),
            dma((n_tp // n_fs,)),
            dma,
            dma((n_z,)),
            dma,
            dma((n_fs, CHUNKS)),
            dma,
            dma,
            dma((3, len(DUAL))),
            dma,
            dma,
            dma((n_tp, QUARTERS)),
            dma,
            dma((n_tp,)),
            dma,
            dma((n_tp,)),
        ],
        compiler_params=pltpu.CompilerParams(
            collective_id=0, has_side_effects=True, vmem_limit_bytes=51 * 1024 * 1024
        ),
    )(tokens, norm_gain[None, :], gate_train, up_train, down_train)
    return pl.pallas_call(
        write_out,
        out_shape=(
            jax.ShapeDtypeStruct((rows * n_fs, cols), BF16),
            jax.ShapeDtypeStruct((rows * n_fs, cols), BF16),
            jax.ShapeDtypeStruct((tall, width * n_tp), BF16),
            jax.ShapeDtypeStruct((piece_rows, width * n_tp), BF16),
        ),
        in_specs=[vmem] * 3,
        out_specs=(pl.BlockSpec(memory_space=pl.ANY),) * 4,
        scratch_shapes=[dma((2, n_fs)), dma((n_tp,)), dma],
        compiler_params=pltpu.CompilerParams(vmem_limit_bytes=4 * 1024 * 1024),
    )(weights, down, layer)


def plain(tokens, norm_gain, gate_train, up_train, down_train):
    gate_local = (norm_gain[:, None] * gate_train).astype(BF16)
    up_local = (norm_gain[:, None] * up_train).astype(BF16)
    down_local = down_train.astype(BF16)
    features = lax.all_gather(tokens, "tp", axis=1, tiled=True)
    wide = features.astype(F32)
    squares = jnp.sum(wide * wide, axis=1)
    gate_whole = lax.all_gather(gate_local, "fs", axis=0, tiled=True)
    up_whole = lax.all_gather(up_local, "fs", axis=0, tiled=True)
    gate_sum = jnp.dot(features, gate_whole, preferred_element_type=F32)
    up_sum = jnp.dot(features, up_whole, preferred_element_type=F32)
    down_rows = lax.all_gather(down_local, "fs", axis=0, tiled=True)
    down_whole = lax.all_to_all(down_rows, "tp", split_axis=0, concat_axis=1, tiled=True)
    scale = lax.rsqrt(squares / features.shape[1] + epsilon)[:, None]
    hidden = (jax.nn.silu(gate_sum * scale) * (up_sum * scale)).astype(BF16)
    mixed = lax.psum_scatter(
        jnp.dot(hidden, down_whole, preferred_element_type=F32).astype(BF16), "tp", scatter_dimension=0, tiled=True
    )
    return (gate_whole, up_whole, down_whole, mixed)


def solution(mesh):
    n_fs, n_tp = mesh.shape["fs"], mesh.shape["tp"]
    fast = n_fs == 4 and n_tp == 8
    return jax.shard_map(
        functools.partial(body, n_fs=n_fs, n_tp=n_tp) if fast else plain,
        mesh=mesh,
        in_specs=(P("fs", "tp"), P("fs"), P("fs", "tp"), P("fs", "tp"), P("fs", "tp")),
        out_specs=(P(None, "tp"), P(None, "tp"), P("tp", None), P(("fs", "tp"), None)),
        check_vma=False,
    )
```

```python
import functools

import jax
import jax.numpy as jnp
from jax import lax
from jax.experimental import pallas as pl
from jax.experimental.pallas import tpu as pltpu
from jax.sharding import PartitionSpec as P

MESH = pl.DeviceIdType.MESH
BF16 = jnp.bfloat16
F32 = jnp.float32
epsilon = 1e-06
CHUNKS = 4
X_ORDER = (0, 2, 1, 3)
Y_ORDER = (1, 3, 0, 2)
QUARTERS = 4
CHAIN_SHARE = 5
DUAL = (0, 1)
CHAIN = (2, 3)
scope = jax.named_scope


def flip(a, k):
    result = 0
    for bit in (1, 2, 4):
        own, other = (a // bit) % 2, (k // bit) % 2
        result = result + bit * (own + other - 2 * own * other)
    return result


def kernel(
    tok_in, gain_in, gate_in, up_in, down_in,
    wbuf, dbuf, layer_out,
    gain, w32, d32, dcast, xbuf, tbuf, acc, hidden, scale, keep, psend, precv, zsend, zrecv,
    load_g, load_t, load_w, load_d, tok_s, tok_r, w_s, w_r, dz_s, o_s, o_r, zr_s, d_s, d_r, p_s, p_r, z_s, z_r,
):
    f, t = lax.axis_index("fs"), lax.axis_index("tp")
    n_tp, n_fs = tbuf.shape[0], wbuf.shape[1]
    z, core = t // 2, t % 2
    fx, fy, fd = flip(f, 1), flip(f, 2), flip(f, 3)
    mate = flip(t, 1)
    base = t - core
    rows = wbuf.shape[2]
    part = rows // CHUNKS
    w_ins = (gate_in, up_in)
    tall, width = dbuf.shape[1], dbuf.shape[2]
    short = tall * CHAIN_SHARE // 32
    long = tall // 2 - short
    per = n_tp // n_fs
    n_tok = tbuf.shape[1]
    piece_rows = n_tok // n_tp
    n_z = n_tp // 2
    q = flip(f, z)
    side = jnp.logical_or(q == 1, q == 2)
    toward = fx + (fy - fx) * (q // 2)
    away = fy + (fx - fy) * (q // 2)

    def remote(src, dst, ss, rs, to_f, to_t):
        return pltpu.make_async_remote_copy(
            src_ref=src, dst_ref=dst, send_sem=ss, recv_sem=rs, device_id=(to_f, to_t), device_id_type=MESH
        )

    def load(w, i):
        return pltpu.make_async_copy(w_ins[w].at[pl.ds(i * part, part)], w32.at[w, pl.ds(i * part, part)], load_w.at[w, i])

    barrier = pltpu.get_barrier_semaphore()
    peers = [(fx, t), (fy, t)] + [(f, flip(t, k)) for k in range(1, n_tp)]
    for peer in peers:
        pl.semaphore_signal(barrier, inc=1, device_id=peer, device_id_type=MESH)

    load_gain = pltpu.make_async_copy(gain_in, gain, load_g)
    load_tok = pltpu.make_async_copy(tok_in, tbuf.at[t], load_t)
    load_down = [
        pltpu.make_async_copy(down_in.at[pl.ds(c * tall, tall)], d32.at[pl.ds(c * tall, tall)], load_d.at[c])
        for c in range(per)
    ]
    load_gain.start()
    for i in (0, 1):
        for w in range(2):
            load(w, i).start()
    load_tok.start()
    for copy in load_down:
        copy.start()
    for i in (2, 3):
        for w in range(2):
            load(w, i).start()

    def cast(w, i):
        block = pl.ds(i * part, part)
        load(w, i).wait()
        lanes = 128
        tall_gain = jnp.broadcast_to(gain[:, block], (lanes, part)).T
        for j in range(wbuf.shape[3] // lanes):
            columns = pl.ds(j * lanes, lanes)
            wbuf[w, f, block, columns] = (tall_gain * w32[w, block, columns]).astype(BF16)

    def tok_copy(piece, dz, to):
        return remote(tbuf.at[piece], tbuf.at[piece], tok_s, tok_r.at[dz], f, to)

    def w_copy(src, i, to):
        ref = wbuf.at[:, src, pl.ds(i * part, part)]
        return remote(ref, ref, w_s, w_r.at[src, i], to, t)

    def send_x(step):
        w_copy(f, X_ORDER[step], fx).start()

    def send_y(step):
        w_copy(f, Y_ORDER[step], fy).start()

    def send_own(step):
        send_x(step)
        send_y(step)

    def rows_of(h):
        return pl.ds(h * long, long) if h in DUAL else pl.ds(2 * long + (h - 2) * short, short)

    def dz_copy(c, h):
        return remote(dcast.at[c, rows_of(h)], dbuf.at[t, rows_of(h)], dz_s, d_r.at[t, h], f, f * per + c)

    def o_copy(slot, h, to):
        return remote(dcast.at[:, rows_of(h)], xbuf.at[slot, :, rows_of(h)], o_s, o_r.at[slot, h], to, t)

    def transit(h, to):
        ref = xbuf.at[2, :, rows_of(h)]
        return remote(ref, ref, o_s, o_r.at[2, h], to, t)

    def over_z(slot, c, h, column):
        return remote(xbuf.at[slot, c, rows_of(h)], dbuf.at[t, rows_of(h)], zr_s, d_r.at[t, h], f, column * per + c)

    def d_copy(piece, h, to):
        ref = dbuf.at[piece, rows_of(h)]
        return remote(ref, ref, d_s, d_r.at[piece, h], to, t)

    def sent(ref, sem):
        remote(ref, ref, sem, sem, fx, t).wait_send()

    chain_stops = (q == 2, q == 1)
    chain_to = (fx + (fy - fx) * (q % 2) * (1 - q // 2), fy + (fx - fy) * (1 - q % 2) * (q // 2))

    def chain(k, hs):
        piece = flip(base, k)
        for h in hs:
            @pl.when(jnp.logical_not(chain_stops[h % 2]))
            def _():
                if isinstance(k, int) and k < per:
                    @pl.when(jnp.logical_or(q != 0, core != k))
                    def _():
                        d_copy(piece, h, chain_to[h % 2]).wait_recv()
                else:
                    d_copy(piece, h, chain_to[h % 2]).wait_recv()
                d_copy(piece, h, chain_to[h % 2]).start()

    inner = jnp.logical_or(z == 1, z == 2)

    def chain_next(n):
        r = n // 2
        chain(2 * jnp.where(inner, 1 + r, 3 - r) + n % 2, CHAIN)

    def own_chain():
        for k in range(per):
            chain(k, range(QUARTERS))

    def hand(k, h, to):
        piece = flip(base, k)
        d_copy(piece, h, to).wait_recv()
        d_copy(piece, h, to).start()

    load_gain.wait()
    cast(0, X_ORDER[0])
    cast(1, X_ORDER[0])
    with scope("barrier"):
        pl.semaphore_wait(barrier, len(peers))
    cast(0, Y_ORDER[0])
    send_x(0)
    cast(1, Y_ORDER[0])
    send_y(0)
    load_tok.wait()
    for dz, k in enumerate((1, 2, 4, 6)):
        tok_copy(t, dz, flip(t, k)).start()

    for c in range(per):
        load_down[c].wait()
        for h in range(QUARTERS):
            block = rows_of(h)
            dcast[c, block] = d32[pl.ds(c * tall + block.start, block.size)].astype(BF16)

        @pl.when(t == f * per + c)
        def _():
            dbuf[t] = dcast[c]

    cast(0, X_ORDER[1])
    cast(0, Y_ORDER[1])

    @pl.when(side)
    def _():
        for h in DUAL:
            o_copy(q - 1, h, toward).start()

    @pl.when(q == 3)
    def _():
        o_copy(2, 0, fx).start()
        o_copy(2, 1, fy).start()

    for h in CHAIN + DUAL:
        for c in range(per):
            @pl.when(t != f * per + c)
            def _():
                dz_copy(c, h).start()

    cast(1, X_ORDER[1])
    cast(1, Y_ORDER[1])

    @pl.when(q == 0)
    def _():
        own_chain()

    send_own(1)

    def arrive(step):
        w_copy(fx, X_ORDER[step], fy).wait_recv()
        w_copy(fy, Y_ORDER[step], fx).wait_recv()

    def forward(step):
        w_copy(fx, X_ORDER[step], fy).start()
        w_copy(fy, Y_ORDER[step], fx).start()

    with scope("arrive0"):
        arrive(0)
    with scope("transit"):
        for way in range(2):
            @pl.when(q == 1 + way)
            def _():
                transit(1 - way, toward).wait_recv()
                transit(1 - way, toward).start()
                for c in range(per):
                    over_z(2, c, 1 - way, away).start()

    send_own(2)

    with scope("own_chain"):
        @pl.when(side)
        def _():
            own_chain()

    send_own(3)

    with scope("over_z"):
        @pl.when(q == 0)
        def _():
            for h in DUAL:
                for slot, column in enumerate((fx, fy)):
                    o_copy(slot, h, fx).wait_recv()
                    for c in range(per):
                        over_z(slot, c, h, column).start()

    with scope("arrive1"):
        forward(0)
        arrive(1)

    with scope("over_z2"):
        @pl.when(q == 0)
        def _():
            for h in DUAL:
                o_copy(2, h, fx).wait_recv()
                for c in range(per):
                    over_z(2, c, h, fd).start()

    with scope("chain0"):
        @pl.when(q == 0)
        def _():
            chain_next(0)
            chain_next(1)

    forward(1)

    tile = 512

    def accumulate(src, first, parts=range(per)):
        def one(n, _):
            w, column = n // (wbuf.shape[3] // tile), pl.multiple_of(n % (wbuf.shape[3] // tile) * tile, tile)
            total = 0.0 if first else acc[w, :, pl.ds(column, tile)]
            for p in parts:
                total = total + jnp.dot(
                    tbuf[src * per + p],
                    wbuf[w, src, pl.ds(p * width, width), pl.ds(column, tile)],
                    preferred_element_type=F32,
                )
            acc[w, :, pl.ds(column, tile)] = total
            return 0

        lax.fori_loop(0, 2 * (wbuf.shape[3] // tile), one, 0)

    with scope("tokens"):
        for dz in range(1, n_z):
            piece = flip(t, 2 * dz)
            tok_copy(piece, dz, mate).wait_recv()
            tok_copy(piece, 0, mate).start()
        remote(tbuf.at[pl.ds(0, n_z)], tbuf.at[pl.ds(0, n_z)], tok_s, tok_r.at[0], f, mate).wait_recv()

    with scope("own_chain3"):
        @pl.when(q == 3)
        def _():
            own_chain()

    def norm(i, _):
        block = pl.ds(i * piece_rows, piece_rows)
        squares = 0.0
        for p in range(n_tp):
            wide = tbuf[p, block].astype(F32)
            squares = squares + wide * wide
        scale[block] = lax.rsqrt(jnp.sum(squares, axis=1, keepdims=True) / (n_tp * width) + epsilon)
        return 0

    with scope("norm"):
        lax.fori_loop(0, n_tp, norm, 0)
    with scope("own_dot"):
        accumulate(f, True)
    with scope("arrive23"):
        for step in range(CHUNKS // 2, CHUNKS):
            arrive(step)
    with scope("fx_dot"):
        accumulate(fx, False)
    with scope("fy_dot"):
        accumulate(fy, False)

    with scope("early"):
        @pl.when(q == 0)
        def _():
            for n in range(2, 6):
                chain_next(n)
            for k, to in ((4, fx), (5, fx), (2, fy), (3, fy)):
                for h in DUAL:
                    hand(k, h, to)

        for place, k, to in ((1, 2, fy), (2, 4, fx)):
            @pl.when(q == place)
            def _():
                chain_next(0)
                chain_next(1)
                for h in DUAL:
                    hand(k, h, to)
                    d_copy(flip(base, k + 1), h, to).wait_recv()

        @pl.when(q == 3)
        def _():
            hand(6, 0, fx)
            hand(6, 1, fy)

    for p in range(per):
        with scope("fd_wait"):
            for i in (2 * p, 2 * p + 1):
                w_copy(fd, i, fx).wait_recv()
        if p < per - 1:
            with scope("fd_dot"):
                accumulate(fd, False, (p,))

    def make_hidden(n, _):
        columns = pl.ds(pl.multiple_of(n * tile, tile), tile)
        s = scale[...]
        g, u = [
            (acc[w, :, columns] + jnp.dot(
                tbuf[fd * per + per - 1],
                wbuf[w, fd, pl.ds((per - 1) * width, width), columns],
                preferred_element_type=F32,
            )) * s
            for w in range(2)
        ]
        hidden[:, columns] = (g / (1.0 + jnp.exp(-g)) * u).astype(BF16)
        return 0

    with scope("hidden"):
        lax.fori_loop(0, hidden.shape[1] // tile, make_hidden, 0)

    def p_copy(k):
        return remote(psend.at[k], precv.at[k], p_s, p_r.at[k], f, mate)

    def z_copy(k, dz, piece):
        to = flip(t, 2 * dz)
        return remote(zsend.at[k, to // 2], zrecv.at[z, piece], z_s, z_r.at[piece], f, to)

    def finish(k):
        p_copy(k).wait_recv()
        for b in range(n_z):
            zsend[k, b] = (keep[k, b] + precv[k, b].astype(F32)).astype(BF16)
        piece = flip(base, k)
        zrecv[z, piece] = zsend[k, z]
        far = jnp.where(inner, 2, 3)
        for dz in (far, 5 - far, 1):
            z_copy(k, dz, piece).start()

    def product(k):
        piece = flip(base, k)
        out = jnp.dot(hidden[...], dbuf[piece], preferred_element_type=F32)
        out = out.reshape(n_z, 2, piece_rows, width)

        @pl.when(core == 0)
        def _():
            keep[k] = out[:, 0]
            psend[k] = out[:, 1].astype(BF16)

        @pl.when(core == 1)
        def _():
            keep[k] = out[:, 1]
            psend[k] = out[:, 0].astype(BF16)

        p_copy(k).start()

    def take(k):
        piece = flip(base, k)
        r = k // 2
        passed = jnp.logical_or(
            jnp.logical_or(jnp.logical_and(r == 1, q < 2), jnp.logical_and(r == 2, q % 2 == 0)),
            jnp.logical_and(r == 3, q == 3),
        )

        @pl.when(jnp.logical_and(r > 0, jnp.logical_not(passed)))
        def _():
            for h in DUAL:
                d_copy(piece, h, fx).wait_recv()

        for side_h in range(2):
            @pl.when(chain_stops[side_h])
            def _():
                d_copy(piece, CHAIN[side_h], fx).wait_recv()

                @pl.when(r == 0)
                def _():
                    d_copy(piece, DUAL[side_h], fx).wait_recv()

    def turn(i):
        k = i
        for here, order in (
            (jnp.logical_and(inner, q == 1), (0, 1, 2, 3, 4, 6, 5, 7)),
            (jnp.logical_and(inner, q == 2), (0, 1, 2, 4, 5, 6, 3, 7)),
            (jnp.logical_and(inner, q == 3), (0, 1, 2, 4, 6, 7, 3, 5)),
            (jnp.logical_and(jnp.logical_not(inner), q % 2 == 0), (0, 1, 6, 7, 4, 5, 2, 3)),
            (jnp.logical_and(jnp.logical_not(inner), q % 2 == 1), (0, 1, 6, 7, 4, 2, 5, 3)),
        ):
            mine = 0
            for n, v in enumerate(order):
                mine = mine + v * jnp.where(i == n, 1, 0)
            k = jnp.where(here, mine, k)
        return k

    def pass_on(i):
        @pl.when(jnp.logical_and(side, i == 2))
        def _():
            for n in range(2, 6):
                chain_next(n)

        for place, k, to in ((1, 3, fy), (2, 5, fx)):
            @pl.when(jnp.logical_and(q == place, i == 2))
            def _():
                for h in DUAL:
                    d_copy(flip(base, k), h, to).start()

        @pl.when(jnp.logical_and(q == 3, i == 2))
        def _():
            chain_next(0)
            chain_next(1)
            hand(7, 0, fx)
            hand(7, 1, fy)

        @pl.when(jnp.logical_and(q == 3, jnp.logical_and(i >= 3, i <= 4)))
        def _():
            chain_next(2 * i - 4)
            chain_next(2 * i - 3)

    def step(i, _):
        with scope("pass_on"):
            pass_on(i)

        last = i - 1 - jnp.where(jnp.logical_or(q == 0, i >= n_tp), 1, 0)
        now = jnp.logical_or(q == 0, i != n_tp - 1)

        @pl.when(jnp.logical_and(now, jnp.logical_and(last >= 0, last < n_tp)))
        def _():
            with scope("finish"):
                finish(turn(last))

        @pl.when(i < n_tp)
        def _():
            k = turn(i)
            with scope("take"):
                take(k)
            with scope("product"):
                product(k)

        return 0

    lax.fori_loop(0, n_tp + 2, step, 0)

    with scope("sent"):
        sent(tbuf.at[pl.ds(0, n_tp - 1)], tok_s)
        sent(wbuf.at[:, pl.ds(0, n_fs - 1)], w_s)
        sent(psend, p_s)

        @pl.when(q == 0)
        def _():
            sent(dcast.at[0], dz_s)
            sent(xbuf, zr_s)
            sent(dbuf.at[:, pl.ds(0, 3 * tall // 4 + short // 2)], d_s)

        @pl.when(side)
        def _():
            sent(xbuf.at[:, :, rows_of(0)], o_s)
            sent(xbuf.at[0, 0], zr_s)
            sent(dbuf.at[:, pl.ds(0, 3 * tall // 8 + short // 4)], d_s)

        @pl.when(q == 3)
        def _():
            sent(xbuf.at[0], o_s)
            sent(dbuf.at[:, pl.ds(0, tall // 2 + short)], d_s)

        @pl.when(q != 0)
        def _():
            sent(dcast, dz_s)

    for piece in range(n_tp):
        with scope("z_wait"):
            others = zrecv.at[pl.ds(0, n_z - 1), piece]
            remote(others, others, z_s, z_r.at[piece], f, mate).wait_recv()
        total = zrecv[0, piece].astype(F32)
        for b in range(1, n_z):
            total = total + zrecv[b, piece].astype(F32)
        layer_out[:, pl.ds(piece * width, width)] = total.astype(BF16)
    sent(zsend.at[:, pl.ds(0, n_z - 1)], z_s)


def write_out(weights, down, layer, gate_out, up_out, down_out, layer_out, w_s, d_s, l_s):
    _, n_fs, rows, _ = weights.shape
    n_tp, _, width = down.shape
    copies = [pltpu.make_async_copy(layer, layer_out, l_s)]
    for w, out in enumerate((gate_out, up_out)):
        for src in range(n_fs):
            copies.append(pltpu.make_async_copy(weights.at[w, src], out.at[pl.ds(src * rows, rows)], w_s.at[w, src]))
    for j in range(n_tp):
        copies.append(pltpu.make_async_copy(down.at[j], down_out.at[:, pl.ds(j * width, width)], d_s.at[j]))
    for copy in copies:
        copy.start()
    for copy in copies:
        copy.wait()


def body(tokens, norm_gain, gate_train, up_train, down_train, *, n_fs, n_tp):
    n_tok, width = tokens.shape
    rows, cols = gate_train.shape
    tall = down_train.shape[0] * n_fs // n_tp
    piece_rows = n_tok // n_tp
    n_z = n_tp // 2
    hbm = pl.BlockSpec(memory_space=pltpu.HBM)
    vmem = pl.BlockSpec(memory_space=pltpu.VMEM)
    dma = pltpu.SemaphoreType.DMA
    weights, down, layer = pl.pallas_call(
        kernel,
        out_shape=(
            pltpu.VMEM((2, n_fs, rows, cols), BF16),
            pltpu.VMEM((n_tp, tall, width), BF16),
            pltpu.VMEM((piece_rows, width * n_tp), BF16),
        ),
        in_specs=[hbm] * 5,
        out_specs=(vmem, vmem, vmem),
        scratch_shapes=[
            pltpu.VMEM((1, rows), F32),
            pltpu.VMEM((2, rows, cols), F32),
            pltpu.VMEM(down_train.shape, F32),
            pltpu.VMEM((n_tp // n_fs, tall, width), BF16),
            pltpu.VMEM((3, n_tp // n_fs, tall - tall * CHAIN_SHARE // 16, width), BF16),
            pltpu.VMEM((n_tp, n_tok, width), BF16),
            pltpu.VMEM((2, n_tok, cols), F32),
            pltpu.VMEM((n_tok, cols), BF16),
            pltpu.VMEM((n_tok, 1), F32),
            pltpu.VMEM((n_tp, n_z, piece_rows, width), F32),
            pltpu.VMEM((n_tp, n_z, piece_rows, width), BF16),
            pltpu.VMEM((n_tp, n_z, piece_rows, width), BF16),
            pltpu.VMEM((n_tp, n_z, piece_rows, width), BF16),
            pltpu.VMEM((n_z, n_tp, piece_rows, width), BF16),
            dma,
            dma,
            dma((2, CHUNKS)),
            dma((n_tp // n_fs,)),
            dma,
            dma((n_z,)),
            dma,
            dma((n_fs, CHUNKS)),
            dma,
            dma,
            dma((3, len(DUAL))),
            dma,
            dma,
            dma((n_tp, QUARTERS)),
            dma,
            dma((n_tp,)),
            dma,
            dma((n_tp,)),
        ],
        compiler_params=pltpu.CompilerParams(
            collective_id=0, has_side_effects=True, vmem_limit_bytes=51 * 1024 * 1024
        ),
    )(tokens, norm_gain[None, :], gate_train, up_train, down_train)
    return pl.pallas_call(
        write_out,
        out_shape=(
            jax.ShapeDtypeStruct((rows * n_fs, cols), BF16),
            jax.ShapeDtypeStruct((rows * n_fs, cols), BF16),
            jax.ShapeDtypeStruct((tall, width * n_tp), BF16),
            jax.ShapeDtypeStruct((piece_rows, width * n_tp), BF16),
        ),
        in_specs=[vmem] * 3,
        out_specs=(pl.BlockSpec(memory_space=pl.ANY),) * 4,
        scratch_shapes=[dma((2, n_fs)), dma((n_tp,)), dma],
        compiler_params=pltpu.CompilerParams(vmem_limit_bytes=4 * 1024 * 1024),
    )(weights, down, layer)


def plain(tokens, norm_gain, gate_train, up_train, down_train):
    gate_local = (norm_gain[:, None] * gate_train).astype(BF16)
    up_local = (norm_gain[:, None] * up_train).astype(BF16)
    down_local = down_train.astype(BF16)
    features = lax.all_gather(tokens, "tp", axis=1, tiled=True)
    wide = features.astype(F32)
    squares = jnp.sum(wide * wide, axis=1)
    gate_whole = lax.all_gather(gate_local, "fs", axis=0, tiled=True)
    up_whole = lax.all_gather(up_local, "fs", axis=0, tiled=True)
    gate_sum = jnp.dot(features, gate_whole, preferred_element_type=F32)
    up_sum = jnp.dot(features, up_whole, preferred_element_type=F32)
    down_rows = lax.all_gather(down_local, "fs", axis=0, tiled=True)
    down_whole = lax.all_to_all(down_rows, "tp", split_axis=0, concat_axis=1, tiled=True)
    scale = lax.rsqrt(squares / features.shape[1] + epsilon)[:, None]
    hidden = (jax.nn.silu(gate_sum * scale) * (up_sum * scale)).astype(BF16)
    mixed = lax.psum_scatter(
        jnp.dot(hidden, down_whole, preferred_element_type=F32).astype(BF16), "tp", scatter_dimension=0, tiled=True
    )
    return (gate_whole, up_whole, down_whole, mixed)


def solution(mesh):
    n_fs, n_tp = mesh.shape["fs"], mesh.shape["tp"]
    fast = n_fs == 4 and n_tp == 8
    return jax.shard_map(
        functools.partial(body, n_fs=n_fs, n_tp=n_tp) if fast else plain,
        mesh=mesh,
        in_specs=(P("fs", "tp"), P("fs"), P("fs", "tp"), P("fs", "tp"), P("fs", "tp")),
        out_specs=(P(None, "tp"), P(None, "tp"), P("tp", None), P(("fs", "tp"), None)),
        check_vma=False,
    )
```
